512 devices in a mesh: sp: 64 (over z, y), tp: 8 (over x, core).
Axes of the slice: x: 4, y: 4, z: 16, core: 2. Of those that a mesh axis runs over, the one named last changes fastest.
Arguments:
- tokens: bfloat16 [4096, 1, 2048], P('sp'), may hold values from -6 to 6
- queries: bfloat16 [4096, 1, 1024], P('sp', None, 'tp'), may hold values from -15 to 15
- key_values: bfloat16 [4096, 1, 1024], P('sp', None, 'tp'), may hold values from -6 to 6
- stop_bias: bfloat16 [4096, 1, 16], P('sp', None, 'tp'), may hold values from -20 to 0
- out_proj: bfloat16 [1024, 2048], P('tp'), may hold values from -0.375 to 0.375
- norm_gain: float32 [2048], replicated, may hold values from 0.1 to 1.9
- up_proj: bfloat16 [2048, 4096], P('sp', 'tp'), may hold values from -0.125 to 0.125
- down_proj: bfloat16 [4096, 2048], P('tp', 'sp'), may hold values from -0.09375 to 0.09375
Outputs:
- layer_out: bfloat16 [4096, 1, 2048], P(('sp', 'tp'))
The draws below stay inside these ranges and needn't reach their ends.
All inputs are finite; a program needn't handle non-finite values.
Results may differ from the reference program's by a relative error of at most 0.018.
Values may be sent and summed in bfloat16 or wider, within the bound.
A program may use at most 64 MiB of HBM per device.

```python
import jax
import jax.numpy as jnp
from jax import lax

D = 2048
FF = 4096
QUERY_HEAD_COUNT = 16
KV_HEADS = 8
HEAD = 64
SEQUENCE_COUNT = 1
TOK_DEV = 64
TOKEN_LENGTH = 4096
N_TP = 8


def draw_stop_bias(key, part):
    key_tensor = jax.random.split(key, 7)
    fast_heads = jax.random.randint(key_tensor[0], (SEQUENCE_COUNT, QUERY_HEAD_COUNT), 0, 2) == 0
    slow_level = -jnp.log(jnp.float32(TOKEN_LENGTH)) - jax.random.uniform(key_tensor[1], (SEQUENCE_COUNT, QUERY_HEAD_COUNT), minval=2.5, maxval=4.0)
    fast_level = -jax.random.uniform(key_tensor[2], (SEQUENCE_COUNT, QUERY_HEAD_COUNT), minval=6.0, maxval=7.5)
    base_level = jnp.where(fast_heads, fast_level, slow_level)
    block_count = TOKEN_LENGTH // TOK_DEV
    shifts = jax.random.uniform(key_tensor[3], (SEQUENCE_COUNT, QUERY_HEAD_COUNT, block_count), minval=-0.7, maxval=0.7)
    shifts = jnp.repeat(shifts, TOK_DEV, axis=2)
    rough_part = jax.random.uniform(key_tensor[4], (SEQUENCE_COUNT, QUERY_HEAD_COUNT, TOKEN_LENGTH), minval=-1.0, maxval=1.0)
    tier_levels = base_level[:, :, None] + shifts + rough_part
    stretch_places = jax.random.randint(key_tensor[5], (SEQUENCE_COUNT, QUERY_HEAD_COUNT, 4), 0, TOKEN_LENGTH)
    stretch_matches = jnp.any(jnp.arange(TOKEN_LENGTH)[None, None, :, None] == stretch_places[:, :, None, :], axis=3)
    stretch_groups = jax.random.uniform(key_tensor[6], (SEQUENCE_COUNT, QUERY_HEAD_COUNT, TOKEN_LENGTH), minval=-2.0, maxval=0.0)
    tier_levels = jnp.where(stretch_matches, stretch_groups, tier_levels)
    return jnp.transpose(tier_levels, (2, 0, 1)).astype(jnp.float32).astype(jnp.bfloat16)


def steps_of(key, shape, cuts, smallest, high):
    def one(axis_at, shards_of):
        heights = jax.random.uniform(jax.random.fold_in(jax.random.fold_in(key, 6), axis_at), (shards_of,), jnp.float32, smallest / len(cuts), high / len(cuts))
        return jnp.repeat(jnp.exp(heights), shape[axis_at] // shards_of).reshape((-1,) + (1,) * (len(shape) - axis_at - 1))

    level = one(*cuts[0])
    for cut in cuts[1:]:
        level = level * one(*cut)
    return level


def normal_values(stream_key, extent, scale, most, cuts=(), kind=jnp.bfloat16):
    values = jax.random.normal(stream_key, extent, jnp.float32) * scale
    if len(cuts) > 0:
        values = steps_of(stream_key, extent, cuts, -0.22, 0.18) * values
    return jnp.clip(values, min=-most, max=most).astype(kind)


def setup_inputs(seed: int = 0) -> dict:
    seeds = jax.random.split(jax.random.key(seed), 9)
    tokens = normal_values(seeds[0], (TOKEN_LENGTH, SEQUENCE_COUNT, D), 1.0, 6.0, ((0, 64),))
    queries = normal_values(seeds[1], (TOKEN_LENGTH, SEQUENCE_COUNT, QUERY_HEAD_COUNT * HEAD), 2.5, 15.0, ((0, 64), (2, 8)))
    key_values = normal_values(seeds[2], (TOKEN_LENGTH, SEQUENCE_COUNT, KV_HEADS * 2 * HEAD), 1.0, 6.0, ((0, 64), (2, 8)))
    stop_bias = draw_stop_bias(jax.random.fold_in(seeds[8], 71), 0)
    out_proj = normal_values(seeds[4], (QUERY_HEAD_COUNT * HEAD, D), (QUERY_HEAD_COUNT * HEAD // 4) ** -0.5, 0.375, ((0, 8),))
    norm_gain = jnp.clip(1.0 + 0.18 * jax.random.normal(seeds[5], (D,), jnp.float32), 0.1, 1.9)
    up_proj = normal_values(seeds[6], (D, FF), D ** -0.5, 0.125, ((0, 64), (1, 8)))
    down_proj = normal_values(seeds[7], (FF, D), FF ** -0.5, 0.09375, ((0, 8), (1, 64)))
    return {"tokens": tokens, "queries": queries, "key_values": key_values, "stop_bias": stop_bias, "out_proj": out_proj, "norm_gain": norm_gain, "up_proj": up_proj, "down_proj": down_proj}


EPSILON = 1e-06

def rms_scale(residual, gain):
    values = residual.astype(jnp.float32)
    factor = lax.rsqrt(lax.optimization_barrier(jnp.mean(values * values, axis=-1, keepdims=True)) + EPSILON)
    return (values * factor * gain).astype(jnp.bfloat16)

def reference(tokens, queries, key_values, stop_bias, out_proj, norm_gain, up_proj, down_proj):
    total_rows = tokens.shape[0]
    seq_count = tokens.shape[1]
    group_size = QUERY_HEAD_COUNT // KV_HEADS
    block_count = total_rows // TOK_DEV
    query_heads = queries.reshape(total_rows, seq_count, QUERY_HEAD_COUNT, HEAD).transpose(1, 2, 0, 3)
    query_heads = query_heads.reshape(seq_count * QUERY_HEAD_COUNT, total_rows, HEAD)
    kv_pairs = key_values.reshape(total_rows, seq_count, KV_HEADS, 2 * HEAD).transpose(1, 2, 0, 3)
    biases = jnp.transpose(stop_bias, (1, 2, 0)).astype(jnp.float32)
    positions = jnp.arange(total_rows, dtype=jnp.int32)

    def one_head(inputs):
        flat_index, q_head = inputs
        seq_index = flat_index // QUERY_HEAD_COUNT
        head_index = flat_index % QUERY_HEAD_COUNT
        kv_pair = kv_pairs[seq_index, head_index // group_size]
        keys_part = kv_pair[:, :HEAD]
        values_part = kv_pair[:, HEAD:]
        bias_row = biases[seq_index, head_index]
        q_blocks = q_head.reshape(block_count, TOK_DEV, HEAD)

        def one_block(block_inputs):
            number, q_block = block_inputs
            scores = jnp.dot(q_block, jnp.transpose(keys_part), preferred_element_type=jnp.float32) * 0.125 + bias_row[None, :]
            query_pos = number * TOK_DEV + jnp.arange(TOK_DEV, dtype=jnp.int32)
            strict = positions[None, :] < query_pos[:, None]
            log_pass = jnp.where(strict, jax.nn.log_sigmoid(-scores), 0.0)
            after_sum = lax.cumsum(log_pass, axis=1, reverse=True) - log_pass
            weights = jnp.where(strict, jnp.exp(jax.nn.log_sigmoid(scores) + after_sum), 0.0).astype(jnp.bfloat16)
            return jnp.dot(weights, values_part, preferred_element_type=jnp.float32).astype(jnp.bfloat16)
        outputs = lax.map(one_block, (jnp.arange(block_count, dtype=jnp.int32), q_blocks))
        return outputs.reshape(total_rows, HEAD)
    attended = lax.map(one_head, (jnp.arange(seq_count * QUERY_HEAD_COUNT, dtype=jnp.int32), query_heads))
    attended = attended.reshape(seq_count, QUERY_HEAD_COUNT, total_rows, HEAD).transpose(2, 0, 1, 3)
    attended = attended.reshape(total_rows * seq_count, QUERY_HEAD_COUNT * HEAD)
    head_width = QUERY_HEAD_COUNT * HEAD // N_TP
    projected = jnp.zeros((total_rows * seq_count, D), jnp.float32)
    for group_index in range(N_TP):
        lower = group_index * head_width
        partial_value = jnp.dot(attended[:, lower:lower + head_width], out_proj[lower:lower + head_width], preferred_element_type=jnp.float32)
        projected = projected + lax.optimization_barrier(partial_value.astype(jnp.bfloat16)).astype(jnp.float32)
    flat_tokens = tokens.reshape(total_rows * seq_count, D)
    residual = (flat_tokens.astype(jnp.float32) + projected).astype(jnp.bfloat16)
    normed = rms_scale(residual, norm_gain)
    hidden = jnp.square(jax.nn.relu(jnp.dot(normed, up_proj, preferred_element_type=jnp.float32))).astype(jnp.bfloat16)
    unit_width = FF // N_TP
    update = jnp.zeros((total_rows * seq_count, D), jnp.float32)
    for group_index in range(N_TP):
        lower = group_index * unit_width
        partial_value = jnp.dot(hidden[:, lower:lower + unit_width], down_proj[lower:lower + unit_width], preferred_element_type=jnp.float32)
        update = update + lax.optimization_barrier(partial_value.astype(jnp.bfloat16)).astype(jnp.float32)
    result = (residual.astype(jnp.float32) + update).astype(jnp.bfloat16)
    return result.reshape(total_rows, seq_count, D)
```

```python
import jax
import jax.numpy as jnp
from jax import lax
from jax.experimental import pallas as pl
from jax.experimental.pallas import tpu as pltpu
from jax.sharding import PartitionSpec as P

MESH = pl.DeviceIdType.MESH
NZ, NY, NX, NC = 16, 4, 4, 2
NCHIP = NX * NY
HEAD = 64
ROWS = 64
D = 2048
HALF = D // 2
EPSILON = 1e-06
LOG2E = 1.4426950408889634
UP_STEPS, DOWN_STEPS = 8, 7


def nn(a, b):
    return lax.dot_general(a, b, (((1,), (0,)), ((), ())), preferred_element_type=jnp.float32)


def nt(a, b):
    return lax.dot_general(a, b, (((1,), (1,)), ((), ())), preferred_element_type=jnp.float32)


def tn(a, b):
    return lax.dot_general(a, b, (((0,), (0,)), ((), ())), preferred_element_type=jnp.float32)


def kernel(
    tok_ref, q_ref, kv_ref, bias_ref, wo_ref, gain_ref, up_ref, down_ref, out_ref,
    kvall, wbuf, wcat, pbuf, prec, xbuf, e1, e1r, own, e2, erec,
    u_hi, s_hi, u_lo, s_lo,
    kv_s, kv_r, yf_s, yf_r, we_s, we_r, w_s, w_r, p_s, p_r, x_s, x_r, xd_s, xd_r, e1_s, e1_r, e_s, e_r,
):
    sp = lax.axis_index("sp")
    tp = lax.axis_index("tp")
    z, y = sp // NY, sp % NY
    x, c = tp // NC, tp % NC
    chip = y * NX + x
    z_next, z_prev = (z + 1) % NZ, (z + NZ - 1) % NZ
    sibling = (sp, x * NC + 1 - c)

    def chip_at(r, core):
        dy, dx = r // NX, r % NX
        return (z * NY + (y + dy) % NY, ((x + dx) % NX) * NC + core)

    def rdma(src, dst, send, recv, device):
        return pltpu.make_async_remote_copy(
            src_ref=src, dst_ref=dst, send_sem=send, recv_sem=recv, device_id=device, device_id_type=MESH
        )

    barrier = pltpu.get_barrier_semaphore()
    peers = [(z_next * NY + y, tp), (z_prev * NY + y, tp), sibling]
    peers += [chip_at(r, c) for r in range(1, NCHIP)]
    peers += [chip_at(r, 1 - c) for r in range(1, NX)]
    for peer in peers:
        pl.semaphore_signal(barrier, inc=1, device_id=peer, device_id_type=MESH)

    kvall[z, y, 0:ROWS, :] = kv_ref[...]
    bias = bias_ref[...].astype(jnp.float32)
    bias = jnp.concatenate([bias, jnp.zeros((14, HEAD), jnp.float32)], axis=0)
    bias = jnp.concatenate([bias, jnp.zeros((16, HEAD), jnp.float32)], axis=1)
    kvall[z, y, ROWS : ROWS + 16, :] = bias.astype(jnp.bfloat16)
    u_hi[...] = jnp.zeros_like(u_hi)
    u_lo[...] = jnp.zeros_like(u_lo)
    s_hi[...] = jnp.zeros_like(s_hi)
    s_lo[...] = jnp.zeros_like(s_lo)

    pl.semaphore_wait(barrier, len(peers))

    def kv_up(k):
        slot = kvall.at[(z - k + 1 + NZ) % NZ, y]
        return rdma(slot, slot, kv_s.at[0, k], kv_r.at[0, k], (z_next * NY + y, tp))

    def kv_down(k):
        slot = kvall.at[(z + k - 1) % NZ, y]
        return rdma(slot, slot, kv_s.at[1, k], kv_r.at[1, k], (z_prev * NY + y, tp))

    def kv_hand(direction, k, p, d):
        slot = kvall.at[p, y]
        return rdma(
            slot, slot, yf_s.at[direction, k, d], yf_r.at[direction, k, d], (z * NY + (y + d) % NY, tp)
        )

    def up_sends(k):
        return (k <= UP_STEPS) & (z - k + 1 >= 0) & (z <= NZ - 2)

    def up_arrives(k):
        return (k <= UP_STEPS) & (z - k >= 0)

    def down_sends(k):
        return (k <= DOWN_STEPS) & ((z + k - 1) % NZ <= DOWN_STEPS - 1)

    def down_arrives(k):
        return (k <= DOWN_STEPS) & ((z + k) % NZ <= DOWN_STEPS - 1)

    def down_used(k):
        return (k <= DOWN_STEPS) & (z + k >= NZ)

    @pl.when(up_sends(1))
    def _():
        kv_up(1).start()

    @pl.when(down_sends(1))
    def _():
        kv_down(1).start()

    for d in range(1, NY):
        kv_hand(0, 0, z, d).start()

    def w_hand(d, which):
        src = (up_ref, down_ref)[which]
        to = (y + d) % NY
        return rdma(
            src.at[:, pl.ds(pl.multiple_of(to * 128, 128), 128)],
            wbuf.at[z, which, pl.ds(pl.multiple_of(y * 32, 32), 32), :],
            we_s.at[d, which], we_r.at[d, which], (z * NY + to, tp),
        )

    for d in range(1, NY):
        for which in range(2):
            w_hand(d, which).start()
    for which in range(2):
        src = (up_ref, down_ref)[which]
        wbuf[z, which, pl.ds(pl.multiple_of(y * 32, 32), 32), :] = src[
            :, pl.ds(pl.multiple_of(y * 128, 128), 128)
        ]

    def w_copy(direction, k):
        p = (z - k + 1 + NZ) % NZ if direction == 0 else (z + k - 1) % NZ
        to = (z_next, z_prev)[direction]
        slot = wbuf.at[p]
        return rdma(slot, slot, w_s.at[direction, k], w_r.at[direction, k], (to * NY + y, tp))

    def w_first():
        for d in range(1, NY):
            for which in range(2):
                w_hand(d, which).wait_recv()
        w_copy(0, 1).start()
        w_copy(1, 1).start()

    def w_step(k):
        w_copy(0, k).wait_recv()
        if k <= DOWN_STEPS:
            w_copy(1, k).wait_recv()
        if k + 1 <= UP_STEPS:
            w_copy(0, k + 1).start()
        if k + 1 <= DOWN_STEPS:
            w_copy(1, k + 1).start()

    q = q_ref[...].astype(jnp.float32) * 0.125
    queries = jnp.concatenate([q[:, :HEAD], q[:, HEAD:]], axis=0).astype(jnp.bfloat16)
    pick = lax.broadcasted_iota(jnp.int32, (16, 128), 1) // HEAD
    pick = (pick == lax.broadcasted_iota(jnp.int32, (16, 128), 0)).astype(jnp.float32).astype(jnp.bfloat16)
    later = lax.broadcasted_iota(jnp.int32, (256, 256), 1) > lax.broadcasted_iota(jnp.int32, (256, 256), 0)
    later = later.astype(jnp.float32).astype(jnp.bfloat16)

    def attend(p, diagonal, carry):
        parts = []
        for b in range(NY):
            keys = kvall[p, b, 0:ROWS, 0:HEAD]
            biases = kvall[p, b, ROWS : ROWS + 16, 0:HEAD]
            parts.append(nt(keys, queries) + tn(biases, pick))
        score = jnp.concatenate(parts, axis=0) * LOG2E
        tail = jnp.log2(1.0 + jnp.exp2(-jnp.abs(score)))
        log_pass = -jnp.maximum(score, 0.0) - tail
        log_stop = jnp.minimum(score, 0.0) - tail
        if diagonal:
            key_at = lax.broadcasted_iota(jnp.int32, (256, 128), 0)
            query_at = y * ROWS + lax.broadcasted_iota(jnp.int32, (256, 128), 1) % HEAD
            strict = key_at < query_at
            log_pass = jnp.where(strict, log_pass, 0.0)
        high = log_pass.astype(jnp.bfloat16)
        low = (log_pass - high.astype(jnp.float32)).astype(jnp.bfloat16)
        after = nn(later, jnp.concatenate([high, low], axis=1))
        after = after[:, :128] + after[:, 128:]
        total = after[0:1, :] + log_pass[0:1, :]
        weights = jnp.exp2(log_stop + (after + carry))
        if diagonal:
            weights = jnp.where(strict, weights, 0.0)
        weights = weights.astype(jnp.bfloat16)
        values = jnp.concatenate([kvall[p, b, 0:ROWS, HEAD:128] for b in range(NY)], axis=0)
        return tn(values, weights), total

    def attend_high(p, diagonal):
        carry = s_hi[0:1, :]
        part, total = attend(p, diagonal, carry)
        u_hi[...] += part
        s_hi[0:1, :] = carry + total

    def attend_low(p):
        part, total = attend(p, False, 0.0)
        u_lo[...] = u_lo[...] * jnp.exp2(total) + part
        s_lo[0:1, :] += total

    def step(k, unused):
        @pl.when(up_arrives(k))
        def _():
            kv_up(k).wait_recv()

        @pl.when(up_sends(k + 1))
        def _():
            kv_up(k + 1).start()

        @pl.when(up_arrives(k))
        def _():
            for d in range(1, NY):
                kv_hand(0, k, (z - k + NZ) % NZ, d).start()

        @pl.when(down_arrives(k))
        def _():
            kv_down(k).wait_recv()

        @pl.when(down_sends(k + 1))
        def _():
            kv_down(k + 1).start()

        @pl.when(down_used(k))
        def _():
            for d in range(1, NY):
                kv_hand(1, k, (z + k) % NZ, d).start()

        @pl.when(k == 2)
        def _():
            w_first()

        for w in range(1, 4):
            @pl.when(k == 2 * w + 2)
            def _():
                w_step(w)

        @pl.when(k == 1)
        def _():
            for d in range(1, NY):
                kv_hand(0, 0, z, d).wait_recv()
            attend_high(z, True)

        @pl.when((k > 1) & (z - k + 1 >= 0))
        def _():
            p = (z - k + 1 + NZ) % NZ
            for d in range(1, NY):
                kv_hand(0, k - 1, p, d).wait_recv()
            attend_high(p, False)

        @pl.when((k > 1) & down_used(k - 1))
        def _():
            p = (z + k - 1) % NZ
            for d in range(1, NY):
                kv_hand(1, k - 1, p, d).wait_recv()
            attend_low(p)

        return unused

    lax.fori_loop(1, UP_STEPS + 2, step, 0)

    mixed = u_hi[...] + u_lo[...] * jnp.exp2(s_hi[0:1, :])
    mixed = mixed.T.astype(jnp.bfloat16)
    w_step(4)

    partial = nn(mixed[:ROWS], wo_ref[0:HEAD, :]) + nn(mixed[ROWS:], wo_ref[HEAD:, :])
    partial = partial.reshape(8, 8, D)
    pbuf[...] = jnp.concatenate([partial[:, :, :HALF], partial[:, :, HALF:]], axis=1).astype(jnp.bfloat16)

    def p_copy(r):
        to = (tp + r) % 8
        return rdma(pbuf.at[to], prec.at[r], p_s.at[r], p_r.at[r], (sp, to))

    for r in range(1, 8):
        p_copy(r).start()
    w_step(5)
    projected = pbuf[tp].astype(jnp.float32)
    for r in range(1, 8):
        p_copy(r).wait_recv()
        projected = projected + prec[r].astype(jnp.float32)
    projected = jnp.concatenate([projected[:8], projected[8:]], axis=1)
    residual = (tok_ref[...].astype(jnp.float32) + projected).astype(jnp.bfloat16).astype(jnp.float32)
    factor = lax.rsqrt(jnp.mean(residual * residual, axis=-1, keepdims=True) + EPSILON)
    normed = residual * factor * gain_ref[...]
    xbuf[c, chip] = jnp.concatenate([normed[:, :HALF], normed[:, HALF:]], axis=0).astype(jnp.bfloat16)

    def x_copy(r):
        slot = xbuf.at[c, chip]
        return rdma(slot, slot, x_s.at[r], x_r.at[r], chip_at(r, c))

    def x_pass(r):
        dy, dx = r // NX, r % NX
        source = ((y + NY - dy) % NY) * NX + (x + NX - dx) % NX
        slot = xbuf.at[c, source]
        return rdma(slot, slot, xd_s.at[r], xd_r.at[r], sibling)

    order = sorted(range(1, NCHIP), key=lambda r: min(r // NX, NY - r // NX) + min(r % NX, NX - r % NX))
    for r in reversed(order):
        x_copy(r).start()
    x_pass(0).start()
    w_step(6)
    w_step(7)
    for r in order:
        x_copy(r).wait_recv()
        x_pass(r).start()
    w_step(8)
    for p in range(8):
        wcat[p * 128 : (p + 1) * 128, 0:128] = wbuf[p, 0]
        wcat[p * 128 : (p + 1) * 128, 128:256] = wbuf[p + 8, 0]
    for r in range(NCHIP):
        x_pass(r).wait_recv()

    def hidden_of(core):
        both = nn(xbuf[core].reshape(NCHIP * 16, HALF), wcat[...]).reshape(NCHIP, 16, 256)
        h = both[:, :8, :128] + both[:, 8:, 128:]
        h = jnp.maximum(h.reshape(NCHIP * 8, 128), 0.0)
        return (h * h).astype(jnp.bfloat16)

    def update_of(h, target, dtype):
        for p in range(8):
            w = jnp.concatenate([wbuf[p, 1], wbuf[p + 8, 1]], axis=0)
            o = nt(h, w).reshape(NCHIP, 8, 256)
            target[:, :, p * 128 : (p + 1) * 128] = jnp.concatenate(
                [o[:, :, :128], o[:, :, 128:]], axis=1
            ).astype(dtype)

    update_of(hidden_of(1 - c), e1, jnp.bfloat16)
    swap = rdma(e1, e1r, e1_s, e1_r, sibling)
    swap.start()
    update_of(hidden_of(c), own, jnp.float32)
    swap.wait_recv()

    def e_copy(r):
        dy, dx = r // NX, r % NX
        target = ((y + dy) % NY) * NX + (x + dx) % NX
        return rdma(e2.at[target], erec.at[r], e_s.at[r], e_r.at[r], chip_at(r, c))

    e2[...] = (own[...] + e1r[...].astype(jnp.float32)).astype(jnp.bfloat16)
    for r in reversed(order):
        e_copy(r).start()
    update = own[chip] + e1r[chip].astype(jnp.float32)
    for r in order:
        e_copy(r).wait_recv()
        update = update + erec[r].astype(jnp.float32)
    update = jnp.concatenate([update[:8], update[8:]], axis=1)
    out_ref[...] = (residual + update).astype(jnp.bfloat16)

    def drain(k, unused):
        @pl.when(up_sends(k))
        def _():
            kv_up(k).wait_send()

        @pl.when(down_sends(k))
        def _():
            kv_down(k).wait_send()

        @pl.when(up_arrives(k))
        def _():
            for d in range(1, NY):
                kv_hand(0, k, (z - k + NZ) % NZ, d).wait_send()

        @pl.when(down_used(k))
        def _():
            for d in range(1, NY):
                kv_hand(1, k, (z + k) % NZ, d).wait_send()

        return unused

    lax.fori_loop(1, UP_STEPS + 1, drain, 0)
    for d in range(1, NY):
        kv_hand(0, 0, z, d).wait_send()
        for which in range(2):
            w_hand(d, which).wait_send()
    for k in range(1, UP_STEPS + 1):
        w_copy(0, k).wait_send()
    for k in range(1, DOWN_STEPS + 1):
        w_copy(1, k).wait_send()
    for r in range(1, 8):
        p_copy(r).wait_send()
    for r in range(NCHIP):
        x_pass(r).wait_send()
    for r in range(1, NCHIP):
        x_copy(r).wait_send()
        e_copy(r).wait_send()
    swap.wait_send()


def body(tokens, queries, key_values, stop_bias, out_proj, norm_gain, up_proj, down_proj):
    tp = lax.axis_index("tp")
    own_tokens = lax.dynamic_slice_in_dim(tokens, tp * 8, 8, 0).reshape(8, D)
    bf, f32 = jnp.bfloat16, jnp.float32
    dma = pltpu.SemaphoreType.DMA
    out = pl.pallas_call(
        kernel,
        out_shape=jax.ShapeDtypeStruct((8, D), bf),
        in_specs=[pl.BlockSpec(memory_space=pltpu.VMEM)] * 8,
        out_specs=pl.BlockSpec(memory_space=pltpu.VMEM),
        scratch_shapes=[
            pltpu.VMEM((NZ, NY, ROWS + 16, 128), bf),
            pltpu.VMEM((NZ, 2, 128, 128), bf),
            pltpu.VMEM((HALF, 256), bf),
            pltpu.VMEM((8, 16, HALF), bf),
            pltpu.VMEM((8, 16, HALF), bf),
            pltpu.VMEM((NC, NCHIP, 16, HALF), bf),
            pltpu.VMEM((NCHIP, 16, HALF), bf),
            pltpu.VMEM((NCHIP, 16, HALF), bf),
            pltpu.VMEM((NCHIP, 16, HALF), f32),
            pltpu.VMEM((NCHIP, 16, HALF), bf),
            pltpu.VMEM((NCHIP, 16, HALF), bf),
            pltpu.VMEM((HEAD, 128), f32),
            pltpu.VMEM((8, 128), f32),
            pltpu.VMEM((HEAD, 128), f32),
            pltpu.VMEM((8, 128), f32),
            dma((2, 9)), dma((2, 9)),
            dma((2, 9, 4)), dma((2, 9, 4)),
            dma((4, 2)), dma((4, 2)),
            dma((2, 9)), dma((2, 9)),
            dma((8,)), dma((8,)),
            dma((NCHIP,)), dma((NCHIP,)),
            dma((NCHIP,)), dma((NCHIP,)),
            dma(()), dma(()),
            dma((NCHIP,)), dma((NCHIP,)),
        ],
        compiler_params=pltpu.CompilerParams(
            collective_id=0, has_side_effects=True, vmem_limit_bytes=40 * 1024 * 1024
        ),
        name="layer",
    )(
        own_tokens,
        queries.reshape(ROWS, 128),
        key_values.reshape(ROWS, 128),
        stop_bias.reshape(ROWS, 2).T,
        out_proj,
        norm_gain.reshape(1, D),
        up_proj,
        down_proj.T,
    )
    return out.reshape(8, 1, D)


def solution(mesh):
    return jax.shard_map(
        body,
        mesh=mesh,
        in_specs=(
            P("sp", None, None),
            P("sp", None, "tp"),
            P("sp", None, "tp"),
            P("sp", None, "tp"),
            P("tp", None),
            P(),
            P("sp", "tp"),
            P("tp", "sp"),
        ),
        out_specs=P(("sp", "tp"), None, None),
        check_vma=False,
    )
```

```python
import jax
import jax.numpy as jnp
from jax import lax
from jax.experimental import pallas as pl
from jax.experimental.pallas import tpu as pltpu
from jax.sharding import PartitionSpec as P

MESH = pl.DeviceIdType.MESH
NZ, NY, NX, NC = 16, 4, 4, 2
NCHIP = NX * NY
HEAD = 64
ROWS = 64
D = 2048
HALF = D // 2
EPSILON = 1e-06
LOG2E = 1.4426950408889634
UP_STEPS, DOWN_STEPS = 8, 7


def nn(a, b):
    return lax.dot_general(a, b, (((1,), (0,)), ((), ())), preferred_element_type=jnp.float32)


def nt(a, b):
    return lax.dot_general(a, b, (((1,), (1,)), ((), ())), preferred_element_type=jnp.float32)


def tn(a, b):
    return lax.dot_general(a, b, (((0,), (0,)), ((), ())), preferred_element_type=jnp.float32)


def kernel(
    tok_hbm, q_hbm, kv_hbm, bias_hbm, wo_hbm, gain_hbm, up_hbm, down_hbm, out_ref,
    tok_ref, q_ref, bias_ref, wo_ref, gain_ref, up_ref, down_ref, in_s,
    kvall, wbuf, wcat, pbuf, prec, xbuf, e1, e1r, own, e2, erec,
    u_hi, s_hi, u_lo, s_lo,
    kv_s, kv_r, yf_s, yf_r, we_s, we_r, w_s, w_r, p_s, p_r, x_s, x_r, xd_s, xd_r, e1_s, e1_r, e_s, e_r,
):
    sp = lax.axis_index("sp")
    tp = lax.axis_index("tp")
    z, y = sp // NY, sp % NY
    x, c = tp // NC, tp % NC
    chip = y * NX + x
    sibling = (sp, x * NC + 1 - c)

    def chip_at(r, core):
        dy, dx = r // NX, r % NX
        return (z * NY + (y + dy) % NY, ((x + dx) % NX) * NC + core)

    def rdma(src, dst, send, recv, device):
        return pltpu.make_async_remote_copy(
            src_ref=src, dst_ref=dst, send_sem=send, recv_sem=recv, device_id=device, device_id_type=MESH
        )

    barrier = pltpu.get_barrier_semaphore()
    peers = [(((z + d) % NZ) * NY + y, tp) for d in (1, 2, NZ - 2, NZ - 1)] + [sibling]
    peers += [chip_at(r, c) for r in range(1, NCHIP)]
    peers += [chip_at(r, 1 - c) for r in range(1, NX)]
    for peer in peers:
        pl.semaphore_signal(barrier, inc=1, device_id=peer, device_id_type=MESH)

    loads = [
        pltpu.make_async_copy(src, dst, in_s.at[i])
        for i, (src, dst) in enumerate(
            (
                (kv_hbm, kvall.at[z, y, 0:ROWS, :]),
                (bias_hbm, bias_ref),
                (up_hbm, up_ref),
                (down_hbm, down_ref),
                (q_hbm, q_ref),
                (wo_hbm, wo_ref),
                (tok_hbm.at[pl.ds(pl.multiple_of(tp * 8, 8), 8), :], tok_ref),
                (gain_hbm, gain_ref),
            )
        )
    ]
    for load in loads:
        load.start()

    loads[1].wait()
    bias = bias_ref[...].astype(jnp.float32)
    bias = jnp.concatenate([bias, jnp.zeros((14, HEAD), jnp.float32)], axis=0)
    bias = jnp.concatenate([bias, jnp.zeros((16, HEAD), jnp.float32)], axis=1)
    kvall[z, y, ROWS : ROWS + 16, :] = bias.astype(jnp.bfloat16)
    u_hi[...] = jnp.zeros_like(u_hi)
    u_lo[...] = jnp.zeros_like(u_lo)
    s_hi[...] = jnp.zeros_like(s_hi)
    s_lo[...] = jnp.zeros_like(s_lo)

    loads[0].wait()
    pl.semaphore_wait(barrier, len(peers))

    def along(buffer, send, recv, direction, d):
        odd = d % 2
        held = d - 2 + odd
        hop = 2 - odd
        if direction == 0:
            p, to = (z - held + NZ) % NZ, (z + hop) % NZ
        else:
            p, to = (z + held) % NZ, (z - hop + NZ) % NZ
        slot = buffer(p)
        return rdma(slot, slot, send.at[direction, d], recv.at[direction, d], (to * NY + y, tp))

    def kv_copy(direction, d):
        return along(lambda p: kvall.at[p, y], kv_s, kv_r, direction, d)

    def kv_hand(direction, k, p, d):
        slot = kvall.at[p, y]
        return rdma(
            slot, slot, yf_s.at[direction, k, d], yf_r.at[direction, k, d], (z * NY + (y + d) % NY, tp)
        )

    def used(direction, d):
        return (z - d >= 0) if direction == 0 else (z + d >= NZ) & (d <= DOWN_STEPS)

    def place(direction, d):
        return (z - d + NZ) % NZ if direction == 0 else (z + d) % NZ

    def even_sends(direction, d):
        if direction == 0:
            return (d <= UP_STEPS) & (z - d + 2 >= 0) & (z + 2 < NZ)
        return (d <= DOWN_STEPS) & ((z + d - 2) % NZ < DOWN_STEPS)

    def even_arrives(direction, d):
        if direction == 0:
            return (d <= UP_STEPS) & (z - d >= 0)
        return (d <= DOWN_STEPS) & ((z + d) % NZ < DOWN_STEPS)

    def odd_sends(direction, d):
        if direction == 0:
            return (d <= UP_STEPS) & (z - d + 1 >= 0) & (z + 1 < NZ)
        return (d <= DOWN_STEPS) & ((z + NZ - 1) % NZ + d >= NZ)

    def odd_arrives(direction, d):
        return (d <= UP_STEPS) & used(direction, d)

    def kv_stage_sends(direction, j):
        @pl.when(even_sends(direction, 2 * j))
        def _():
            kv_copy(direction, 2 * j).start()

        @pl.when(odd_sends(direction, 2 * j - 1))
        def _():
            kv_copy(direction, 2 * j - 1).start()

    kv_stage_sends(0, 1)
    kv_stage_sends(1, 1)
    for d in range(1, NY):
        kv_hand(0, 0, z, d).start()

    def w_hand(d, which):
        src = (up_ref, down_ref)[which]
        to = (y + d) % NY
        return rdma(
            src.at[:, pl.ds(pl.multiple_of(to * 128, 128), 128)],
            wbuf.at[z, which, pl.ds(pl.multiple_of(y * 32, 32), 32), :],
            we_s.at[d, which], we_r.at[d, which], (z * NY + to, tp),
        )

    loads[2].wait()
    loads[3].wait()
    for d in range(1, NY):
        for which in range(2):
            w_hand(d, which).start()
    for which in range(2):
        src = (up_ref, down_ref)[which]
        wbuf[z, which, pl.ds(pl.multiple_of(y * 32, 32), 32), :] = src[
            :, pl.ds(pl.multiple_of(y * 128, 128), 128)
        ]

    def w_copy(direction, d):
        return along(lambda p: wbuf.at[p], w_s, w_r, direction, d)

    def w_far(j):
        for direction, last in ((0, UP_STEPS), (1, DOWN_STEPS)):
            if 2 * j <= last:
                if j == 0:
                    if direction == 0:
                        for d in range(1, NY):
                            for which in range(2):
                                w_hand(d, which).wait_recv()
                else:
                    w_copy(direction, 2 * j).wait_recv()
            if 2 * j + 2 <= last:
                w_copy(direction, 2 * j + 2).start()

    def w_near(j):
        for direction, last in ((0, UP_STEPS), (1, DOWN_STEPS)):
            if 2 * j + 1 <= last:
                w_copy(direction, 2 * j + 1).start()

    def w_rest():
        for d in range(1, UP_STEPS, 2):
            w_copy(0, d).wait_recv()
            w_copy(1, d).wait_recv()

    loads[4].wait()
    q = q_ref[...].astype(jnp.float32) * 0.125
    queries = jnp.concatenate([q[:, :HEAD], q[:, HEAD:]], axis=0).astype(jnp.bfloat16)
    pick = lax.broadcasted_iota(jnp.int32, (16, 128), 1) // HEAD
    pick = (pick == lax.broadcasted_iota(jnp.int32, (16, 128), 0)).astype(jnp.float32).astype(jnp.bfloat16)
    later = lax.broadcasted_iota(jnp.int32, (256, 256), 1) > lax.broadcasted_iota(jnp.int32, (256, 256), 0)
    later = later.astype(jnp.float32).astype(jnp.bfloat16)

    def attend(p, diagonal, carry):
        parts = []
        for b in range(NY):
            keys = kvall[p, b, 0:ROWS, 0:HEAD]
            biases = kvall[p, b, ROWS : ROWS + 16, 0:HEAD]
            parts.append(nt(keys, queries) + tn(biases, pick))
        score = jnp.concatenate(parts, axis=0) * LOG2E
        tail = jnp.log2(1.0 + jnp.exp2(-jnp.abs(score)))
        log_pass = -jnp.maximum(score, 0.0) - tail
        log_stop = jnp.minimum(score, 0.0) - tail
        if diagonal:
            key_at = lax.broadcasted_iota(jnp.int32, (256, 128), 0)
            query_at = y * ROWS + lax.broadcasted_iota(jnp.int32, (256, 128), 1) % HEAD
            strict = key_at < query_at
            log_pass = jnp.where(strict, log_pass, 0.0)
        high = log_pass.astype(jnp.bfloat16)
        low = (log_pass - high.astype(jnp.float32)).astype(jnp.bfloat16)
        after = nn(later, jnp.concatenate([high, low], axis=1))
        after = after[:, :128] + after[:, 128:]
        total = after[0:1, :] + log_pass[0:1, :]
        weights = jnp.exp2(log_stop + (after + carry))
        if diagonal:
            weights = jnp.where(strict, weights, 0.0)
        weights = weights.astype(jnp.bfloat16)
        values = jnp.concatenate([kvall[p, b, 0:ROWS, HEAD:128] for b in range(NY)], axis=0)
        return tn(values, weights), total

    def attend_high(p, diagonal):
        carry = s_hi[0:1, :]
        part, total = attend(p, diagonal, carry)
        u_hi[...] += part
        s_hi[0:1, :] = carry + total

    def attend_low(p):
        part, total = attend(p, False, 0.0)
        u_lo[...] = u_lo[...] * jnp.exp2(total) + part
        s_lo[0:1, :] += total

    def step(j, unused):
        for direction in range(2):
            @pl.when(even_arrives(direction, 2 * j))
            def _():
                kv_copy(direction, 2 * j).wait_recv()

            kv_stage_sends(direction, j + 1)

            @pl.when((2 * j <= UP_STEPS) & used(direction, 2 * j))
            def _():
                for d in range(1, NY):
                    kv_hand(direction, 2 * j, place(direction, 2 * j), d).start()

            @pl.when(odd_arrives(direction, 2 * j - 1))
            def _():
                kv_copy(direction, 2 * j - 1).wait_recv()
                for d in range(1, NY):
                    kv_hand(direction, 2 * j - 1, place(direction, 2 * j - 1), d).start()

        @pl.when(j == 2)
        def _():
            w_far(0)

        @pl.when(j == 3)
        def _():
            w_near(0)

        @pl.when(j == 4)
        def _():
            w_far(1)

        @pl.when(j == 1)
        def _():
            for d in range(1, NY):
                kv_hand(0, 0, z, d).wait_recv()
            attend_high(z, True)

        for back in (3, 2):
            k = 2 * j - back

            @pl.when((k > 0) & used(0, k))
            def _():
                for d in range(1, NY):
                    kv_hand(0, k, place(0, k), d).wait_recv()
                attend_high(place(0, k), False)

            @pl.when((k > 0) & used(1, k))
            def _():
                for d in range(1, NY):
                    kv_hand(1, k, place(1, k), d).wait_recv()
                attend_low(place(1, k))

        return unused

    lax.fori_loop(1, UP_STEPS // 2 + 2, step, 0)
    w_near(1)
    w_far(2)

    for load in loads[5:]:
        load.wait()

    mixed = u_hi[...] + u_lo[...] * jnp.exp2(s_hi[0:1, :])
    mixed = mixed.T.astype(jnp.bfloat16)

    partial = nn(mixed[:ROWS], wo_ref[0:HEAD, :]) + nn(mixed[ROWS:], wo_ref[HEAD:, :])
    partial = partial.reshape(8, 8, D)
    pbuf[...] = jnp.concatenate([partial[:, :, :HALF], partial[:, :, HALF:]], axis=1).astype(jnp.bfloat16)

    def p_copy(r):
        to = (tp + r) % 8
        return rdma(pbuf.at[to], prec.at[r], p_s.at[r], p_r.at[r], (sp, to))

    for r in range(1, 8):
        p_copy(r).start()
    w_near(2)
    w_far(3)
    w_near(3)
    projected = pbuf[tp].astype(jnp.float32)
    for r in range(1, 8):
        p_copy(r).wait_recv()
        projected = projected + prec[r].astype(jnp.float32)
    projected = jnp.concatenate([projected[:8], projected[8:]], axis=1)
    residual = (tok_ref[...].astype(jnp.float32) + projected).astype(jnp.bfloat16).astype(jnp.float32)
    factor = lax.rsqrt(jnp.mean(residual * residual, axis=-1, keepdims=True) + EPSILON)
    normed = residual * factor * gain_ref[...]
    xbuf[c, chip] = jnp.concatenate([normed[:, :HALF], normed[:, HALF:]], axis=0).astype(jnp.bfloat16)

    def x_copy(r):
        slot = xbuf.at[c, chip]
        return rdma(slot, slot, x_s.at[r], x_r.at[r], chip_at(r, c))

    def x_pass(r):
        dy, dx = r // NX, r % NX
        source = ((y + NY - dy) % NY) * NX + (x + NX - dx) % NX
        slot = xbuf.at[c, source]
        return rdma(slot, slot, xd_s.at[r], xd_r.at[r], sibling)

    rows_order = (2, 1, 3, 0)
    for dy in rows_order:
        for dx in (2, 1, 3, 0):
            if dy or dx:
                x_copy(dy * NX + dx).start()
    x_pass(0).start()
    w_far(4)
    w_rest()
    for p in range(8):
        wcat[p * 128 : (p + 1) * 128, 0:128] = wbuf[p, 0]
        wcat[p * 128 : (p + 1) * 128, 128:256] = wbuf[p + 8, 0]

    def row_of(dy):
        return pl.ds(pl.multiple_of(((y + NY - dy) % NY) * NX, NX), NX)

    def swap(dy):
        rows = row_of(dy)
        return rdma(e1.at[rows], e1r.at[rows], e1_s.at[dy], e1_r.at[dy], sibling)

    def e_copy(r):
        dy, dx = r // NX, r % NX
        target = ((y + dy) % NY) * NX + (x + dx) % NX
        return rdma(e2.at[target], erec.at[r], e_s.at[r], e_r.at[r], chip_at(r, c))

    def feed_forward(dy):
        for dx in (1, 3, 2, 0):
            if dy or dx:
                x_copy(dy * NX + dx).wait_recv()
                x_pass(dy * NX + dx).start()
        for dx in range(NX):
            x_pass(dy * NX + dx).wait_recv()
        rows = row_of(dy)
        both = jnp.concatenate([xbuf[1 - c, rows], xbuf[c, rows]], axis=0).reshape(2 * NX * 16, HALF)
        both = nn(both, wcat[...]).reshape(2 * NX, 16, 256)
        h = both[:, :8, :128] + both[:, 8:, 128:]
        h = jnp.maximum(h.reshape(2 * NX * 8, 128), 0.0)
        h = (h * h).astype(jnp.bfloat16)
        for p in range(8):
            w = jnp.concatenate([wbuf[p, 1], wbuf[p + 8, 1]], axis=0)
            o = nt(h, w).reshape(2 * NX, 8, 256)
            o = jnp.concatenate([o[:, :, :128], o[:, :, 128:]], axis=1)
            e1[rows, :, p * 128 : (p + 1) * 128] = o[:NX].astype(jnp.bfloat16)
            own[rows, :, p * 128 : (p + 1) * 128] = o[NX:]
        swap(dy).start()

    def send_back(dy):
        swap(dy).wait_recv()
        rows = row_of(dy)
        e2[rows] = (own[rows] + e1r[rows].astype(jnp.float32)).astype(jnp.bfloat16)
        for dx in (2, 1, 3, 0):
            r = ((NY - dy) % NY) * NX + dx
            if r:
                e_copy(r).start()

    for n, dy in enumerate(rows_order):
        feed_forward(dy)
        if n:
            send_back(rows_order[n - 1])
    send_back(rows_order[-1])
    update = own[chip] + e1r[chip].astype(jnp.float32)
    for dy in rows_order:
        for dx in range(NX):
            r = ((NY - dy) % NY) * NX + dx
            if r:
                e_copy(r).wait_recv()
                update = update + erec[r].astype(jnp.float32)
    update = jnp.concatenate([update[:8], update[8:]], axis=1)
    out_ref[...] = (residual + update).astype(jnp.bfloat16)

    def drain(j, unused):
        for direction in range(2):
            @pl.when(even_sends(direction, 2 * j))
            def _():
                kv_copy(direction, 2 * j).wait_send()

            @pl.when(odd_sends(direction, 2 * j - 1))
            def _():
                kv_copy(direction, 2 * j - 1).wait_send()

            for k in (2 * j - 1, 2 * j):
                @pl.when(used(direction, k))
                def _():
                    for d in range(1, NY):
                        kv_hand(direction, k, place(direction, k), d).wait_send()

        return unused

    lax.fori_loop(1, UP_STEPS // 2 + 1, drain, 0)
    for d in range(1, NY):
        kv_hand(0, 0, z, d).wait_send()
        for which in range(2):
            w_hand(d, which).wait_send()
    for k in range(1, UP_STEPS + 1):
        w_copy(0, k).wait_send()
    for k in range(1, DOWN_STEPS + 1):
        w_copy(1, k).wait_send()
    for r in range(1, 8):
        p_copy(r).wait_send()
    for r in range(NCHIP):
        x_pass(r).wait_send()
    for r in range(1, NCHIP):
        x_copy(r).wait_send()
        e_copy(r).wait_send()
    for dy in range(NY):
        swap(dy).wait_send()


def body(tokens, queries, key_values, stop_bias, out_proj, norm_gain, up_proj, down_proj):
    bf, f32 = jnp.bfloat16, jnp.float32
    dma = pltpu.SemaphoreType.DMA
    out = pl.pallas_call(
        kernel,
        out_shape=jax.ShapeDtypeStruct((8, D), bf),
        in_specs=[pl.BlockSpec(memory_space=pltpu.HBM)] * 8,
        out_specs=pl.BlockSpec(memory_space=pltpu.VMEM),
        scratch_shapes=[
            pltpu.VMEM((8, D), bf),
            pltpu.VMEM((ROWS, 128), bf),
            pltpu.VMEM((2, HEAD), bf),
            pltpu.VMEM((128, D), bf),
            pltpu.VMEM((1, D), f32),
            pltpu.VMEM((32, 512), bf),
            pltpu.VMEM((32, 512), bf),
            dma((8,)),
            pltpu.VMEM((NZ, NY, ROWS + 16, 128), bf),
            pltpu.VMEM((NZ, 2, 128, 128), bf),
            pltpu.VMEM((HALF, 256), bf),
            pltpu.VMEM((8, 16, HALF), bf),
            pltpu.VMEM((8, 16, HALF), bf),
            pltpu.VMEM((NC, NCHIP, 16, HALF), bf),
            pltpu.VMEM((NCHIP, 16, HALF), bf),
            pltpu.VMEM((NCHIP, 16, HALF), bf),
            pltpu.VMEM((NCHIP, 16, HALF), f32),
            pltpu.VMEM((NCHIP, 16, HALF), bf),
            pltpu.VMEM((NCHIP, 16, HALF), bf),
            pltpu.VMEM((HEAD, 128), f32),
            pltpu.VMEM((8, 128), f32),
            pltpu.VMEM((HEAD, 128), f32),
            pltpu.VMEM((8, 128), f32),
            dma((2, 9)), dma((2, 9)),
            dma((2, 9, 4)), dma((2, 9, 4)),
            dma((4, 2)), dma((4, 2)),
            dma((2, 9)), dma((2, 9)),
            dma((8,)), dma((8,)),
            dma((NCHIP,)), dma((NCHIP,)),
            dma((NCHIP,)), dma((NCHIP,)),
            dma((NY,)), dma((NY,)),
            dma((NCHIP,)), dma((NCHIP,)),
        ],
        compiler_params=pltpu.CompilerParams(
            collective_id=0, has_side_effects=True
        ),
        name="layer",
    )(
        tokens.reshape(ROWS, D),
        queries.reshape(ROWS, 128),
        key_values.reshape(ROWS, 128),
        stop_bias.reshape(ROWS, 2).T,
        out_proj,
        norm_gain.reshape(1, D),
        up_proj,
        down_proj.T,
    )
    return out.reshape(8, 1, D)


def solution(mesh):
    return jax.shard_map(
        body,
        mesh=mesh,
        in_specs=(
            P("sp", None, None),
            P("sp", None, "tp"),
            P("sp", None, "tp"),
            P("sp", None, "tp"),
            P("tp", None),
            P(),
            P("sp", "tp"),
            P("tp", "sp"),
        ),
        out_specs=P(("sp", "tp"), None, None),
        check_vma=False,
    )
```

```python
import jax
import jax.numpy as jnp
from jax import lax
from jax.experimental import pallas as pl
from jax.experimental.pallas import tpu as pltpu
from jax.sharding import PartitionSpec as P

MESH = pl.DeviceIdType.MESH
NZ, NY, NX, NC = 16, 4, 4, 2
NCHIP = NX * NY
HEAD = 64
ROWS = 64
D = 2048
HALF = D // 2
EPSILON = 1e-06
LOG2E = 1.4426950408889634
UP_STEPS, DOWN_STEPS = 8, 7
JUMP = 4
W_PLAN = {0: ((1, 0),), 2: ((0, 0),), 3: ((1, 1),), 5: ((1, 2), (0, 1)), 6: ((0, 2),), 7: ((1, 3), (0, 3))}


def nn(a, b):
    return lax.dot_general(a, b, (((1,), (0,)), ((), ())), preferred_element_type=jnp.float32)


def nt(a, b):
    return lax.dot_general(a, b, (((1,), (1,)), ((), ())), preferred_element_type=jnp.float32)


def tn(a, b):
    return lax.dot_general(a, b, (((0,), (0,)), ((), ())), preferred_element_type=jnp.float32)


def kernel(
    tok_hbm, q_hbm, kv_hbm, bias_hbm, wo_hbm, gain_hbm, up_hbm, down_hbm, out_ref,
    tok_ref, q_ref, bias_ref, wo_ref, gain_ref, up_ref, down_ref, in_s,
    kvall, wbuf, wcat, pbuf, prec, xbuf, e1, e1r, own, e2, erec,
    u_hi, s_hi, u_lo,
    kv_s, kv_r, yf_s, yf_r, we_s, we_r, w_s, w_r, p_s, p_r, x_s, x_r, xd_s, xd_r, e1_s, e1_r, e_s, e_r,
):
    sp = lax.axis_index("sp")
    tp = lax.axis_index("tp")
    z, y = sp // NY, sp % NY
    x, c = tp // NC, tp % NC
    chip = y * NX + x
    sibling = (sp, x * NC + 1 - c)

    def chip_at(r, core):
        dy, dx = r // NX, r % NX
        return (z * NY + (y + dy) % NY, ((x + dx) % NX) * NC + core)

    def rdma(src, dst, send, recv, device):
        return pltpu.make_async_remote_copy(
            src_ref=src, dst_ref=dst, send_sem=send, recv_sem=recv, device_id=device, device_id_type=MESH
        )

    barrier = pltpu.get_barrier_semaphore()
    peers = [(((z + d + NZ) % NZ) * NY + y, tp) for d in range(-JUMP, JUMP + 1) if d] + [sibling]
    peers += [chip_at(r, c) for r in range(1, NCHIP)]
    peers += [chip_at(r, 1 - c) for r in range(1, NX)]
    for peer in peers:
        pl.semaphore_signal(barrier, inc=1, device_id=peer, device_id_type=MESH)

    loads = [
        pltpu.make_async_copy(src, dst, in_s.at[i])
        for i, (src, dst) in enumerate(
            (
                (kv_hbm, kvall.at[z, y, 0:ROWS, :]),
                (bias_hbm, bias_ref),
                (up_hbm, up_ref),
                (down_hbm, down_ref),
                (q_hbm, q_ref),
                (wo_hbm, wo_ref),
                (tok_hbm.at[pl.ds(pl.multiple_of(tp * 8, 8), 8), :], tok_ref),
                (gain_hbm, gain_ref),
            )
        )
    ]
    for load in loads:
        load.start()

    loads[1].wait()
    bias = bias_ref[...].astype(jnp.float32)
    bias = jnp.concatenate([bias, jnp.zeros((14, HEAD), jnp.float32)], axis=0)
    bias = jnp.concatenate([bias, jnp.zeros((16, HEAD), jnp.float32)], axis=1)
    kvall[z, y, ROWS : ROWS + 16, :] = bias.astype(jnp.bfloat16)
    u_lo[...] = jnp.zeros_like(u_lo)

    loads[0].wait()
    pl.semaphore_wait(barrier, len(peers))

    def along(slot_of, send, recv, direction, d, held):
        hop = d - held
        if direction == 0:
            p, to = (z - held + NZ) % NZ, (z + hop) % NZ
        else:
            p, to = (z + held) % NZ, (z - hop + NZ) % NZ
        slot = slot_of(p)
        return rdma(slot, slot, send.at[direction, d], recv.at[direction, d], (to * NY + y, tp))

    def held_at(d):
        return (d - 1) // JUMP * JUMP

    def kv_copy(direction, d):
        return along(lambda p: kvall.at[p, y], kv_s, kv_r, direction, d, held_at(d))

    def used(direction, d):
        return (z - d >= 0) if direction == 0 else (z + d >= NZ) & (d <= DOWN_STEPS)

    def place(direction, d):
        return (z - d + NZ) % NZ if direction == 0 else (z + d) % NZ

    def kv_sends(direction, d):
        held = held_at(d)
        if direction == 0:
            return (z - held >= 0) & (z + d - held < NZ)
        if d % JUMP == 0:
            return (z + held) % NZ < DOWN_STEPS
        return (z - d + held + NZ) % NZ + d >= NZ

    def kv_arrives(direction, d):
        if direction == 1 and d % JUMP == 0:
            return (z + d) % NZ < DOWN_STEPS
        return used(direction, d)

    def kv_steps(direction):
        return range(1, (UP_STEPS, DOWN_STEPS)[direction] + 1)

    def kv_start(direction, d):
        @pl.when(kv_sends(direction, d))
        def _():
            kv_copy(direction, d).start()

    def kv_hand(direction, k, p, d, source=None):
        slot = kvall.at[p, y if source is None else source]
        return rdma(
            slot, slot, yf_s.at[direction, k, d], yf_r.at[direction, k, d], (z * NY + (y + d) % NY, tp)
        )

    def hand_start(direction, k, p):
        kv_hand(direction, k, p, 1).start()
        kv_hand(direction, k, p, 3).start()

        @pl.when(c == 0)
        def _():
            kv_hand(direction, k, p, 2).start()

    def relay(direction, k, p):
        return rdma(
            kvall.at[p, (y + 1) % NY], kvall.at[p, (y + 1) % NY],
            yf_s.at[direction, k, 2], yf_r.at[direction, k, 2], (z * NY + (y + 3) % NY, tp),
        )

    def hand_relay(direction, k, p):
        @pl.when(c == 1)
        def _():
            kv_hand(direction, k, p, 3).wait_recv()
            relay(direction, k, p).start()

    def hand_wait(direction, k, p):
        kv_hand(direction, k, p, 1).wait_recv()

        @pl.when(c == 0)
        def _():
            kv_hand(direction, k, p, 3).wait_recv()

        kv_hand(direction, k, p, 2).wait_recv()

    for d in range(JUMP, 0, -1):
        kv_start(0, d)
        kv_start(1, d)
    hand_start(0, 0, z)

    def w_hand(d, which):
        src = (up_ref, down_ref)[which]
        to = (y + d) % NY
        return rdma(
            src.at[:, pl.ds(pl.multiple_of(to * 128, 128), 128)],
            wbuf.at[z, which, pl.ds(pl.multiple_of(y * 32, 32), 32), :],
            we_s.at[d, which], we_r.at[d, which], (z * NY + to, tp),
        )

    loads[2].wait()
    loads[3].wait()
    for d in range(1, NY):
        for which in range(2):
            w_hand(d, which).start()
    for which in range(2):
        src = (up_ref, down_ref)[which]
        wbuf[z, which, pl.ds(pl.multiple_of(y * 32, 32), 32), :] = src[
            :, pl.ds(pl.multiple_of(y * 128, 128), 128)
        ]

    def w_copy(direction, d):
        return along(lambda p: wbuf.at[p], w_s, w_r, direction, d, (d - 1) // 2 * 2)

    def w_far(j):
        for direction, last in ((0, UP_STEPS), (1, DOWN_STEPS)):
            if 2 * j <= last:
                if j == 0:
                    if direction == 0:
                        for d in range(1, NY):
                            for which in range(2):
                                w_hand(d, which).wait_recv()
                else:
                    w_copy(direction, 2 * j).wait_recv()
            if 2 * j + 2 <= last:
                w_copy(direction, 2 * j + 2).start()

    def w_near(j):
        for direction, last in ((0, UP_STEPS), (1, DOWN_STEPS)):
            if 2 * j + 1 <= last:
                w_copy(direction, 2 * j + 1).start()

    def w_work(point):
        for far, n in W_PLAN.get(point, ()):
            (w_far if far else w_near)(n)

    def w_rest():
        for d in range(1, UP_STEPS, 2):
            w_copy(0, d).wait_recv()
            w_copy(1, d).wait_recv()

    loads[4].wait()
    q = q_ref[...].astype(jnp.float32) * 0.125
    queries = jnp.concatenate([q[:, :HEAD], q[:, HEAD:]], axis=0).astype(jnp.bfloat16)
    pick = lax.broadcasted_iota(jnp.int32, (16, 128), 1) // HEAD
    pick = (pick == lax.broadcasted_iota(jnp.int32, (16, 128), 0)).astype(jnp.float32).astype(jnp.bfloat16)
    later = lax.broadcasted_iota(jnp.int32, (256, 256), 1) > lax.broadcasted_iota(jnp.int32, (256, 256), 0)
    later = later.astype(jnp.float32).astype(jnp.bfloat16)

    def attend(p, diagonal, carry):
        parts = []
        for b in range(NY):
            keys = kvall[p, b, 0:ROWS, 0:HEAD]
            biases = kvall[p, b, ROWS : ROWS + 16, 0:HEAD]
            parts.append(nt(keys, queries) + tn(biases, pick))
        score = jnp.concatenate(parts, axis=0) * LOG2E
        tail = jnp.log2(1.0 + jnp.exp2(-jnp.abs(score)))
        log_pass = -jnp.maximum(score, 0.0) - tail
        log_stop = jnp.minimum(score, 0.0) - tail
        if diagonal:
            key_at = lax.broadcasted_iota(jnp.int32, (256, 128), 0)
            query_at = y * ROWS + lax.broadcasted_iota(jnp.int32, (256, 128), 1) % HEAD
            strict = key_at < query_at
            log_pass = jnp.where(strict, log_pass, 0.0)
        high = log_pass.astype(jnp.bfloat16)
        low = (log_pass - high.astype(jnp.float32)).astype(jnp.bfloat16)
        after = nn(later, jnp.concatenate([high, low], axis=1))
        after = after[:, :128] + after[:, 128:]
        total = after[0:1, :] + log_pass[0:1, :]
        weights = jnp.exp2(log_stop + (after + carry))
        if diagonal:
            weights = jnp.where(strict, weights, 0.0)
        weights = weights.astype(jnp.bfloat16)
        values = jnp.concatenate([kvall[p, b, 0:ROWS, HEAD:128] for b in range(NY)], axis=0)
        return tn(values, weights), total

    def attend_diagonal():
        part, total = attend(z, True, 0.0)
        u_hi[...] = part
        s_hi[0:1, :] = total

    def attend_high(d):
        carry = s_hi[0:1, :]
        part, total = attend(place(0, d), False, carry)
        u_hi[...] += part
        s_hi[0:1, :] = carry + total

    def attend_both(d):
        carry = s_hi[0:1, :]
        part, total = attend(place(0, d), False, carry)
        part_low, total_low = attend(place(1, d), False, 0.0)
        u_hi[...] += part
        s_hi[0:1, :] = carry + total
        u_lo[...] = u_lo[...] * jnp.exp2(total_low) + part_low

    def kv_receive(d):
        for direction in range(2):
            if d in kv_steps(direction):
                @pl.when(kv_arrives(direction, d))
                def _():
                    kv_copy(direction, d).wait_recv()

                if d % JUMP == 0:
                    for further in range(d + JUMP, d, -1):
                        if further in kv_steps(direction):
                            kv_start(direction, further)

                @pl.when(used(direction, d))
                def _():
                    hand_start(direction, d, place(direction, d))

    def relay_step(d, unused):
        for direction in range(2):
            @pl.when(used(direction, d))
            def _():
                hand_relay(direction, d, place(direction, d))

        return unused

    def attend_step(d, unused):
        for direction in range(2):
            @pl.when(used(direction, d))
            def _():
                hand_wait(direction, d, place(direction, d))

        @pl.when(used(1, d))
        def _():
            attend_both(d)

        @pl.when(used(0, d) & jnp.logical_not(used(1, d)))
        def _():
            attend_high(d)

        return unused

    hand_relay(0, 0, z)
    w_work(0)
    for d in (1, 2, 3, 4):
        kv_receive(d)
    w_work(1)
    hand_wait(0, 0, z)
    attend_diagonal()
    lax.fori_loop(1, 5, relay_step, 0)
    w_work(2)
    for d in (5, 6, 7, 8):
        kv_receive(d)
    w_work(3)
    lax.fori_loop(1, 5, attend_step, 0)
    w_work(4)
    lax.fori_loop(5, 9, relay_step, 0)
    w_work(5)
    lax.fori_loop(5, 9, attend_step, 0)
    w_work(6)

    for load in loads[5:]:
        load.wait()

    mixed = u_hi[...] + u_lo[...] * jnp.exp2(s_hi[0:1, :])
    mixed = mixed.T.astype(jnp.bfloat16)

    partial = nn(mixed[:ROWS], wo_ref[0:HEAD, :]) + nn(mixed[ROWS:], wo_ref[HEAD:, :])
    partial = partial.reshape(8, 8, D)
    pbuf[...] = jnp.concatenate([partial[:, :, :HALF], partial[:, :, HALF:]], axis=1).astype(jnp.bfloat16)

    def p_copy(r):
        to = (tp + r) % 8
        return rdma(pbuf.at[to], prec.at[r], p_s.at[r], p_r.at[r], (sp, to))

    for r in range(1, 8):
        p_copy(r).start()
    w_work(7)
    projected = pbuf[tp].astype(jnp.float32)
    for r in range(1, 8):
        p_copy(r).wait_recv()
        projected = projected + prec[r].astype(jnp.float32)
    projected = jnp.concatenate([projected[:8], projected[8:]], axis=1)
    residual = (tok_ref[...].astype(jnp.float32) + projected).astype(jnp.bfloat16).astype(jnp.float32)
    factor = lax.rsqrt(jnp.mean(residual * residual, axis=-1, keepdims=True) + EPSILON)
    normed = residual * factor * gain_ref[...]
    xbuf[c, chip] = jnp.concatenate([normed[:, :HALF], normed[:, HALF:]], axis=0).astype(jnp.bfloat16)

    def x_copy(r):
        slot = xbuf.at[c, chip]
        return rdma(slot, slot, x_s.at[r], x_r.at[r], chip_at(r, c))

    def x_pass(r):
        dy, dx = r // NX, r % NX
        source = ((y + NY - dy) % NY) * NX + (x + NX - dx) % NX
        slot = xbuf.at[c, source]
        return rdma(slot, slot, xd_s.at[r], xd_r.at[r], sibling)

    rows_order = (2, 1, 3, 0)
    for dy in rows_order:
        for dx in (2, 1, 3, 0):
            if dy or dx:
                x_copy(dy * NX + dx).start()
    x_pass(0).start()
    w_work(8)
    for dy in rows_order:
        for dx in (1, 3, 2, 0):
            if dy or dx:
                x_copy(dy * NX + dx).wait_recv()
                x_pass(dy * NX + dx).start()
    w_far(4)
    w_rest()
    for p in range(8):
        wcat[p * 128 : (p + 1) * 128, 0:128] = wbuf[p, 0]
        wcat[p * 128 : (p + 1) * 128, 128:256] = wbuf[p + 8, 0]

    def row_of(dy):
        return pl.ds(pl.multiple_of(((y + NY - dy) % NY) * NX, NX), NX)

    def swap(dy):
        rows = row_of(dy)
        return rdma(e1.at[rows], e1r.at[rows], e1_s.at[dy], e1_r.at[dy], sibling)

    def e_copy(r):
        dy, dx = r // NX, r % NX
        target = ((y + dy) % NY) * NX + (x + dx) % NX
        return rdma(e2.at[target], erec.at[r], e_s.at[r], e_r.at[r], chip_at(r, c))

    def feed_forward(pair):
        for dy in pair:
            for dx in range(NX):
                x_pass(dy * NX + dx).wait_recv()
        tokens = jnp.concatenate([xbuf[core, row_of(dy)] for dy in pair for core in (1 - c, c)], axis=0)
        both = nn(tokens.reshape(4 * NX * 16, HALF), wcat[...]).reshape(4 * NX, 16, 256)
        h = both[:, :8, :128] + both[:, 8:, 128:]
        h = jnp.maximum(h.reshape(4 * NX * 8, 128), 0.0)
        h = (h * h).astype(jnp.bfloat16)
        for p in range(8):
            w = jnp.concatenate([wbuf[p, 1], wbuf[p + 8, 1]], axis=0)
            o = nt(h, w).reshape(4 * NX, 8, 256)
            o = jnp.concatenate([o[:, :, :128], o[:, :, 128:]], axis=1)
            for n, dy in enumerate(pair):
                at = 2 * NX * n
                e1[row_of(dy), :, p * 128 : (p + 1) * 128] = o[at : at + NX].astype(jnp.bfloat16)
                own[row_of(dy), :, p * 128 : (p + 1) * 128] = o[at + NX : at + 2 * NX]
        for dy in pair:
            swap(dy).start()

    def send_back(dy):
        swap(dy).wait_recv()
        rows = row_of(dy)
        e2[rows] = (own[rows] + e1r[rows].astype(jnp.float32)).astype(jnp.bfloat16)
        for dx in (2, 1, 3, 0):
            r = ((NY - dy) % NY) * NX + dx
            if r:
                e_copy(r).start()

    feed_forward(rows_order[:2])
    send_back(rows_order[0])
    send_back(rows_order[1])
    feed_forward(rows_order[2:])
    send_back(rows_order[2])
    send_back(rows_order[3])
    update = own[chip] + e1r[chip].astype(jnp.float32)
    for dy in rows_order:
        for dx in range(NX):
            r = ((NY - dy) % NY) * NX + dx
            if r:
                e_copy(r).wait_recv()
                update = update + erec[r].astype(jnp.float32)
    update = jnp.concatenate([update[:8], update[8:]], axis=1)
    out_ref[...] = (residual + update).astype(jnp.bfloat16)

    for direction in range(2):
        for d in kv_steps(direction):
            @pl.when(kv_sends(direction, d))
            def _():
                kv_copy(direction, d).wait_send()

    def drain(k, unused):
        for direction in range(2):
            @pl.when(used(direction, k))
            def _():
                for d in range(1, NY):
                    kv_hand(direction, k, place(direction, k), d).wait_send()

        return unused

    lax.fori_loop(1, UP_STEPS + 1, drain, 0)
    for d in range(1, NY):
        kv_hand(0, 0, z, d).wait_send()
        for which in range(2):
            w_hand(d, which).wait_send()
    for k in range(1, UP_STEPS + 1):
        w_copy(0, k).wait_send()
    for k in range(1, DOWN_STEPS + 1):
        w_copy(1, k).wait_send()
    for r in range(1, 8):
        p_copy(r).wait_send()
    for r in range(NCHIP):
        x_pass(r).wait_send()
    for r in range(1, NCHIP):
        x_copy(r).wait_send()
        e_copy(r).wait_send()
    for dy in range(NY):
        swap(dy).wait_send()


def body(tokens, queries, key_values, stop_bias, out_proj, norm_gain, up_proj, down_proj):
    bf, f32 = jnp.bfloat16, jnp.float32
    dma = pltpu.SemaphoreType.DMA
    out = pl.pallas_call(
        kernel,
        out_shape=jax.ShapeDtypeStruct((8, D), bf),
        in_specs=[pl.BlockSpec(memory_space=pltpu.HBM)] * 8,
        out_specs=pl.BlockSpec(memory_space=pltpu.VMEM),
        scratch_shapes=[
            pltpu.VMEM((8, D), bf),
            pltpu.VMEM((ROWS, 128), bf),
            pltpu.VMEM((2, HEAD), bf),
            pltpu.VMEM((128, D), bf),
            pltpu.VMEM((1, D), f32),
            pltpu.VMEM((32, 512), bf),
            pltpu.VMEM((32, 512), bf),
            dma((8,)),
            pltpu.VMEM((NZ, NY, ROWS + 16, 128), bf),
            pltpu.VMEM((NZ, 2, 128, 128), bf),
            pltpu.VMEM((HALF, 256), bf),
            pltpu.VMEM((8, 16, HALF), bf),
            pltpu.VMEM((8, 16, HALF), bf),
            pltpu.VMEM((NC, NCHIP, 16, HALF), bf),
            pltpu.VMEM((NCHIP, 16, HALF), bf),
            pltpu.VMEM((NCHIP, 16, HALF), bf),
            pltpu.VMEM((NCHIP, 16, HALF), f32),
            pltpu.VMEM((NCHIP, 16, HALF), bf),
            pltpu.VMEM((NCHIP, 16, HALF), bf),
            pltpu.VMEM((HEAD, 128), f32),
            pltpu.VMEM((8, 128), f32),
            pltpu.VMEM((HEAD, 128), f32),
            dma((2, 9)), dma((2, 9)),
            dma((2, 9, 4)), dma((2, 9, 4)),
            dma((4, 2)), dma((4, 2)),
            dma((2, 9)), dma((2, 9)),
            dma((8,)), dma((8,)),
            dma((NCHIP,)), dma((NCHIP,)),
            dma((NCHIP,)), dma((NCHIP,)),
            dma((NY,)), dma((NY,)),
            dma((NCHIP,)), dma((NCHIP,)),
        ],
        compiler_params=pltpu.CompilerParams(
            collective_id=0, has_side_effects=True
        ),
        name="layer",
    )(
        tokens.reshape(ROWS, D),
        queries.reshape(ROWS, 128),
        key_values.reshape(ROWS, 128),
        stop_bias.reshape(ROWS, 2).T,
        out_proj,
        norm_gain.reshape(1, D),
        up_proj,
        down_proj.T,
    )
    return out.reshape(8, 1, D)


def solution(mesh):
    return jax.shard_map(
        body,
        mesh=mesh,
        in_specs=(
            P("sp", None, None),
            P("sp", None, "tp"),
            P("sp", None, "tp"),
            P("sp", None, "tp"),
            P("tp", None),
            P(),
            P("sp", "tp"),
            P("tp", "sp"),
        ),
        out_specs=P(("sp", "tp"), None, None),
        check_vma=False,
    )
```

```python
import jax
import jax.numpy as jnp
from jax import lax
from jax.experimental import pallas as pl
from jax.experimental.pallas import tpu as pltpu
from jax.sharding import PartitionSpec as P

MESH = pl.DeviceIdType.MESH
NZ, NY, NX, NC = 16, 4, 4, 2
NCHIP = NX * NY
HEAD = 64
ROWS = 64
D = 2048
HALF = D // 2
EPSILON = 1e-06
LOG2E = 1.4426950408889634
UP_STEPS, DOWN_STEPS = 8, 7
JUMP = 4
W_PLAN = {0: ((1, 0),), 1: ((0, 0),), 2: ((1, 1),), 3: ((0, 1),), 5: ((1, 2),), 6: ((0, 2),), 7: ((1, 3), (0, 3))}


def nn(a, b):
    return lax.dot_general(a, b, (((1,), (0,)), ((), ())), preferred_element_type=jnp.float32)


def nt(a, b):
    return lax.dot_general(a, b, (((1,), (1,)), ((), ())), preferred_element_type=jnp.float32)


def tn(a, b):
    return lax.dot_general(a, b, (((0,), (0,)), ((), ())), preferred_element_type=jnp.float32)


def kernel(
    tok_hbm, q_hbm, kv_hbm, bias_hbm, wo_hbm, gain_hbm, up_hbm, down_hbm, out_ref,
    tok_ref, q_ref, bias_ref, wo_ref, gain_ref, up_ref, down_ref, in_s,
    kvall, wbuf, wcat, pbuf, prec, xbuf, e1, e1r, own, e2, erec,
    u_hi, s_hi, u_lo,
    kv_s, kv_r, yf_s, yf_r, we_s, we_r, w_s, w_r, p_s, p_r, x_s, x_r, xd_s, xd_r, e1_s, e1_r, e_s, e_r,
):
    sp = lax.axis_index("sp")
    tp = lax.axis_index("tp")
    z, y = sp // NY, sp % NY
    x, c = tp // NC, tp % NC
    chip = y * NX + x
    sibling = (sp, x * NC + 1 - c)

    def chip_at(r, core):
        dy, dx = r // NX, r % NX
        return (z * NY + (y + dy) % NY, ((x + dx) % NX) * NC + core)

    def rdma(src, dst, send, recv, device):
        return pltpu.make_async_remote_copy(
            src_ref=src, dst_ref=dst, send_sem=send, recv_sem=recv, device_id=device, device_id_type=MESH
        )

    barrier = pltpu.get_barrier_semaphore()
    peers = [(((z + d + NZ) % NZ) * NY + y, tp) for d in range(-JUMP, JUMP + 1) if d] + [sibling]
    peers += [chip_at(r, c) for r in range(1, NCHIP)]
    peers += [chip_at(r, 1 - c) for r in range(1, NX)]
    for peer in peers:
        pl.semaphore_signal(barrier, inc=1, device_id=peer, device_id_type=MESH)

    loads = [
        pltpu.make_async_copy(src, dst, in_s.at[i])
        for i, (src, dst) in enumerate(
            (
                (kv_hbm, kvall.at[z, y, 0:ROWS, :]),
                (bias_hbm, bias_ref),
                (up_hbm, up_ref),
                (down_hbm, down_ref),
                (q_hbm, q_ref),
                (wo_hbm, wo_ref),
                (tok_hbm.at[pl.ds(pl.multiple_of(tp * 8, 8), 8), :], tok_ref),
                (gain_hbm, gain_ref),
            )
        )
    ]
    for load in loads:
        load.start()

    loads[1].wait()
    bias = bias_ref[...].astype(jnp.float32)
    bias = jnp.concatenate([bias, jnp.zeros((14, HEAD), jnp.float32)], axis=0)
    bias = jnp.concatenate([bias, jnp.zeros((16, HEAD), jnp.float32)], axis=1)
    kvall[z, y, ROWS : ROWS + 16, :] = bias.astype(jnp.bfloat16)
    u_lo[...] = jnp.zeros_like(u_lo)

    loads[0].wait()
    pl.semaphore_wait(barrier, len(peers))

    def along(slot_of, send, recv, direction, d, held):
        hop = d - held
        if direction == 0:
            p, to = (z - held + NZ) % NZ, (z + hop) % NZ
        else:
            p, to = (z + held) % NZ, (z - hop + NZ) % NZ
        slot = slot_of(p)
        return rdma(slot, slot, send.at[direction, d], recv.at[direction, d], (to * NY + y, tp))

    def held_at(d):
        return (d - 1) // JUMP * JUMP

    def kv_copy(direction, d):
        return along(lambda p: kvall.at[p, y], kv_s, kv_r, direction, d, held_at(d))

    def used(direction, d):
        return (z - d >= 0) if direction == 0 else (z + d >= NZ) & (d <= DOWN_STEPS)

    def place(direction, d):
        return (z - d + NZ) % NZ if direction == 0 else (z + d) % NZ

    def kv_sends(direction, d):
        held = held_at(d)
        if direction == 0:
            return (z - held >= 0) & (z + d - held < NZ)
        if d % JUMP == 0:
            return (z + held) % NZ < DOWN_STEPS
        return (z - d + held + NZ) % NZ + d >= NZ

    def kv_arrives(direction, d):
        if direction == 1 and d % JUMP == 0:
            return (z + d) % NZ < DOWN_STEPS
        return used(direction, d)

    def kv_steps(direction):
        return range(1, (UP_STEPS, DOWN_STEPS)[direction] + 1)

    def kv_start(direction, d):
        @pl.when(kv_sends(direction, d))
        def _():
            kv_copy(direction, d).start()

    def kv_hand(direction, k, p, d, source=None):
        slot = kvall.at[p, y if source is None else source]
        return rdma(
            slot, slot, yf_s.at[direction, k, d], yf_r.at[direction, k, d], (z * NY + (y + d) % NY, tp)
        )

    def hand_start(direction, k, p):
        kv_hand(direction, k, p, 1).start()
        kv_hand(direction, k, p, 3).start()

        @pl.when(c == 0)
        def _():
            kv_hand(direction, k, p, 2).start()

    def relay(direction, k, p):
        return rdma(
            kvall.at[p, (y + 1) % NY], kvall.at[p, (y + 1) % NY],
            yf_s.at[direction, k, 2], yf_r.at[direction, k, 2], (z * NY + (y + 3) % NY, tp),
        )

    def hand_relay(direction, k, p):
        @pl.when(c == 1)
        def _():
            kv_hand(direction, k, p, 3).wait_recv()
            relay(direction, k, p).start()

    def hand_wait(direction, k, p):
        kv_hand(direction, k, p, 1).wait_recv()

        @pl.when(c == 0)
        def _():
            kv_hand(direction, k, p, 3).wait_recv()

        kv_hand(direction, k, p, 2).wait_recv()

    for d in range(JUMP, 0, -1):
        kv_start(0, d)
        kv_start(1, d)
    hand_start(0, 0, z)

    def w_hand(d, which):
        src = (up_ref, down_ref)[which]
        to = (y + d) % NY
        return rdma(
            src.at[:, pl.ds(pl.multiple_of(to * 128, 128), 128)],
            wbuf.at[z, which, pl.ds(pl.multiple_of(y * 32, 32), 32), :],
            we_s.at[d, which], we_r.at[d, which], (z * NY + to, tp),
        )

    loads[2].wait()
    loads[3].wait()
    for d in range(1, NY):
        for which in range(2):
            w_hand(d, which).start()
    for which in range(2):
        src = (up_ref, down_ref)[which]
        wbuf[z, which, pl.ds(pl.multiple_of(y * 32, 32), 32), :] = src[
            :, pl.ds(pl.multiple_of(y * 128, 128), 128)
        ]

    def w_copy(direction, d):
        return along(lambda p: wbuf.at[p], w_s, w_r, direction, d, (d - 1) // 2 * 2)

    def w_far(j, ways=(0, 1)):
        for direction in ways:
            last = (UP_STEPS, DOWN_STEPS)[direction]
            if 2 * j <= last:
                if j == 0:
                    if direction == ways[0]:
                        for d in range(1, NY):
                            for which in range(2):
                                w_hand(d, which).wait_recv()
                else:
                    w_copy(direction, 2 * j).wait_recv()
            if 2 * j + 2 <= last:
                w_copy(direction, 2 * j + 2).start()

    def w_near(j, ways=(0, 1)):
        for direction in ways:
            last = (UP_STEPS, DOWN_STEPS)[direction]
            if 2 * j + 1 <= last:
                w_copy(direction, 2 * j + 1).start()

    def w_work(point):
        for far, *step in W_PLAN.get(point, ()):
            (w_far if far else w_near)(*step)

    def w_rest():
        for d in range(1, UP_STEPS, 2):
            w_copy(0, d).wait_recv()
            w_copy(1, d).wait_recv()

    loads[4].wait()
    q = q_ref[...].astype(jnp.float32) * 0.125
    queries = jnp.concatenate([q[:, :HEAD], q[:, HEAD:]], axis=0).astype(jnp.bfloat16)
    pick = lax.broadcasted_iota(jnp.int32, (16, 128), 1) // HEAD
    pick = (pick == lax.broadcasted_iota(jnp.int32, (16, 128), 0)).astype(jnp.float32).astype(jnp.bfloat16)
    later = lax.broadcasted_iota(jnp.int32, (256, 256), 1) > lax.broadcasted_iota(jnp.int32, (256, 256), 0)
    later = later.astype(jnp.float32).astype(jnp.bfloat16)

    def attend(p, diagonal, carry):
        parts = []
        for b in range(NY):
            keys = kvall[p, b, 0:ROWS, 0:HEAD]
            biases = kvall[p, b, ROWS : ROWS + 16, 0:HEAD]
            parts.append(nt(keys, queries) + tn(biases, pick))
        score = jnp.concatenate(parts, axis=0) * LOG2E
        tail = jnp.log2(1.0 + jnp.exp2(-jnp.abs(score)))
        log_pass = -jnp.maximum(score, 0.0) - tail
        log_stop = jnp.minimum(score, 0.0) - tail
        if diagonal:
            key_at = lax.broadcasted_iota(jnp.int32, (256, 128), 0)
            query_at = y * ROWS + lax.broadcasted_iota(jnp.int32, (256, 128), 1) % HEAD
            strict = key_at < query_at
            log_pass = jnp.where(strict, log_pass, 0.0)
        high = log_pass.astype(jnp.bfloat16)
        low = (log_pass - high.astype(jnp.float32)).astype(jnp.bfloat16)
        after = nn(later, jnp.concatenate([high, low], axis=1))
        after = after[:, :128] + after[:, 128:]
        total = after[0:1, :] + log_pass[0:1, :]
        weights = jnp.exp2(log_stop + (after + carry))
        if diagonal:
            weights = jnp.where(strict, weights, 0.0)
        weights = weights.astype(jnp.bfloat16)
        values = jnp.concatenate([kvall[p, b, 0:ROWS, HEAD:128] for b in range(NY)], axis=0)
        return tn(values, weights), total

    def attend_diagonal():
        part, total = attend(z, True, 0.0)
        u_hi[...] = part
        s_hi[0:1, :] = total

    def attend_high(d):
        carry = s_hi[0:1, :]
        part, total = attend(place(0, d), False, carry)
        u_hi[...] += part
        s_hi[0:1, :] = carry + total

    def attend_both(d):
        carry = s_hi[0:1, :]
        part, total = attend(place(0, d), False, carry)
        part_low, total_low = attend(place(1, d), False, 0.0)
        u_hi[...] += part
        s_hi[0:1, :] = carry + total
        u_lo[...] = u_lo[...] * jnp.exp2(total_low) + part_low

    def kv_receive(d):
        for direction in range(2):
            if d in kv_steps(direction):
                @pl.when(kv_arrives(direction, d))
                def _():
                    kv_copy(direction, d).wait_recv()

                if d % JUMP == 0:
                    for further in range(d + JUMP, d, -1):
                        if further in kv_steps(direction):
                            kv_start(direction, further)

                @pl.when(used(direction, d))
                def _():
                    hand_start(direction, d, place(direction, d))

    def relay_step(d, unused):
        for direction in range(2):
            @pl.when(used(direction, d))
            def _():
                hand_relay(direction, d, place(direction, d))

        return unused

    def attend_step(d, unused):
        for direction in range(2):
            @pl.when(used(direction, d))
            def _():
                hand_wait(direction, d, place(direction, d))

        @pl.when(used(1, d))
        def _():
            attend_both(d)

        @pl.when(used(0, d) & jnp.logical_not(used(1, d)))
        def _():
            attend_high(d)

        return unused

    hand_relay(0, 0, z)
    w_work(0)
    for d in (1, 2, 3, 4):
        kv_receive(d)
    w_work(1)
    hand_wait(0, 0, z)
    attend_diagonal()
    lax.fori_loop(1, 5, relay_step, 0)
    w_work(2)
    for d in (5, 6, 7, 8):
        kv_receive(d)
    w_work(3)
    lax.fori_loop(1, 5, attend_step, 0)
    w_work(4)
    lax.fori_loop(5, 9, relay_step, 0)
    w_work(5)
    lax.fori_loop(5, 9, attend_step, 0)
    w_work(6)

    for load in loads[5:]:
        load.wait()

    mixed = u_hi[...] + u_lo[...] * jnp.exp2(s_hi[0:1, :])
    mixed = mixed.T.astype(jnp.bfloat16)

    partial = nn(mixed[:ROWS], wo_ref[0:HEAD, :]) + nn(mixed[ROWS:], wo_ref[HEAD:, :])
    partial = partial.reshape(8, 8, D)
    pbuf[...] = jnp.concatenate([partial[:, :, :HALF], partial[:, :, HALF:]], axis=1).astype(jnp.bfloat16)

    def p_copy(r):
        to = (tp + r) % 8
        return rdma(pbuf.at[to], prec.at[r], p_s.at[r], p_r.at[r], (sp, to))

    for r in range(1, 8):
        p_copy(r).start()
    w_work(7)
    projected = pbuf[tp].astype(jnp.float32)
    for r in range(1, 8):
        p_copy(r).wait_recv()
        projected = projected + prec[r].astype(jnp.float32)
    projected = jnp.concatenate([projected[:8], projected[8:]], axis=1)
    residual = (tok_ref[...].astype(jnp.float32) + projected).astype(jnp.bfloat16).astype(jnp.float32)
    factor = lax.rsqrt(jnp.mean(residual * residual, axis=-1, keepdims=True) + EPSILON)
    normed = residual * factor * gain_ref[...]
    xbuf[c, chip] = jnp.concatenate([normed[:, :HALF], normed[:, HALF:]], axis=0).astype(jnp.bfloat16)

    def x_copy(r):
        slot = xbuf.at[c, chip]
        return rdma(slot, slot, x_s.at[r], x_r.at[r], chip_at(r, c))

    def x_pass(r):
        dy, dx = r // NX, r % NX
        source = ((y + NY - dy) % NY) * NX + (x + NX - dx) % NX
        slot = xbuf.at[c, source]
        return rdma(slot, slot, xd_s.at[r], xd_r.at[r], sibling)

    rows_order = (2, 1, 3, 0)
    for dy in rows_order:
        for dx in (2, 1, 3, 0):
            if dy or dx:
                x_copy(dy * NX + dx).start()
    x_pass(0).start()
    w_work(8)
    for dy in rows_order:
        for dx in (1, 3, 2, 0):
            if dy or dx:
                x_copy(dy * NX + dx).wait_recv()
                x_pass(dy * NX + dx).start()
    w_far(4)
    w_rest()
    for p in range(8):
        wcat[p * 128 : (p + 1) * 128, 0:128] = wbuf[p, 0]
        wcat[p * 128 : (p + 1) * 128, 128:256] = wbuf[p + 8, 0]

    def row_of(dy):
        return pl.ds(pl.multiple_of(((y + NY - dy) % NY) * NX, NX), NX)

    def swap(dy):
        rows = row_of(dy)
        return rdma(e1.at[rows], e1r.at[rows], e1_s.at[dy], e1_r.at[dy], sibling)

    def e_copy(r):
        dy, dx = r // NX, r % NX
        target = ((y + dy) % NY) * NX + (x + dx) % NX
        return rdma(e2.at[target], erec.at[r], e_s.at[r], e_r.at[r], chip_at(r, c))

    def feed_forward(pair):
        for dy in pair:
            for dx in range(NX):
                x_pass(dy * NX + dx).wait_recv()
        tokens = jnp.concatenate([xbuf[core, row_of(dy)] for dy in pair for core in (1 - c, c)], axis=0)
        both = nn(tokens.reshape(4 * NX * 16, HALF), wcat[...]).reshape(4 * NX, 16, 256)
        h = both[:, :8, :128] + both[:, 8:, 128:]
        h = jnp.maximum(h.reshape(4 * NX * 8, 128), 0.0)
        h = (h * h).astype(jnp.bfloat16)
        for p in range(8):
            w = jnp.concatenate([wbuf[p, 1], wbuf[p + 8, 1]], axis=0)
            o = nt(h, w).reshape(4 * NX, 8, 256)
            o = jnp.concatenate([o[:, :, :128], o[:, :, 128:]], axis=1)
            for n, dy in enumerate(pair):
                at = 2 * NX * n
                e1[row_of(dy), :, p * 128 : (p + 1) * 128] = o[at : at + NX].astype(jnp.bfloat16)
                own[row_of(dy), :, p * 128 : (p + 1) * 128] = o[at + NX : at + 2 * NX]
        for dy in pair:
            swap(dy).start()

    def send_back(dy):
        swap(dy).wait_recv()
        rows = row_of(dy)
        e2[rows] = (own[rows] + e1r[rows].astype(jnp.float32)).astype(jnp.bfloat16)
        for dx in (2, 1, 3, 0):
            r = ((NY - dy) % NY) * NX + dx
            if r:
                e_copy(r).start()

    feed_forward(rows_order[:2])
    send_back(rows_order[0])
    send_back(rows_order[1])
    feed_forward(rows_order[2:])
    send_back(rows_order[2])
    send_back(rows_order[3])
    update = own[chip] + e1r[chip].astype(jnp.float32)
    for dy in rows_order:
        for dx in range(NX):
            r = ((NY - dy) % NY) * NX + dx
            if r:
                e_copy(r).wait_recv()
                update = update + erec[r].astype(jnp.float32)
    update = jnp.concatenate([update[:8], update[8:]], axis=1)
    out_ref[...] = (residual + update).astype(jnp.bfloat16)

    for direction in range(2):
        for d in kv_steps(direction):
            @pl.when(kv_sends(direction, d))
            def _():
                kv_copy(direction, d).wait_send()

    def drain(k, unused):
        for direction in range(2):
            @pl.when(used(direction, k))
            def _():
                for d in range(1, NY):
                    kv_hand(direction, k, place(direction, k), d).wait_send()

        return unused

    lax.fori_loop(1, UP_STEPS + 1, drain, 0)
    for d in range(1, NY):
        kv_hand(0, 0, z, d).wait_send()
        for which in range(2):
            w_hand(d, which).wait_send()
    for k in range(1, UP_STEPS + 1):
        w_copy(0, k).wait_send()
    for k in range(1, DOWN_STEPS + 1):
        w_copy(1, k).wait_send()
    for r in range(1, 8):
        p_copy(r).wait_send()
    for r in range(NCHIP):
        x_pass(r).wait_send()
    for r in range(1, NCHIP):
        x_copy(r).wait_send()
        e_copy(r).wait_send()
    for dy in range(NY):
        swap(dy).wait_send()


def body(tokens, queries, key_values, stop_bias, out_proj, norm_gain, up_proj, down_proj):
    bf, f32 = jnp.bfloat16, jnp.float32
    dma = pltpu.SemaphoreType.DMA
    out = pl.pallas_call(
        kernel,
        out_shape=jax.ShapeDtypeStruct((8, D), bf),
        in_specs=[pl.BlockSpec(memory_space=pltpu.HBM)] * 8,
        out_specs=pl.BlockSpec(memory_space=pltpu.VMEM),
        scratch_shapes=[
            pltpu.VMEM((8, D), bf),
            pltpu.VMEM((ROWS, 128), bf),
            pltpu.VMEM((2, HEAD), bf),
            pltpu.VMEM((128, D), bf),
            pltpu.VMEM((1, D), f32),
            pltpu.VMEM((32, 512), bf),
            pltpu.VMEM((32, 512), bf),
            dma((8,)),
            pltpu.VMEM((NZ, NY, ROWS + 16, 128), bf),
            pltpu.VMEM((NZ, 2, 128, 128), bf),
            pltpu.VMEM((HALF, 256), bf),
            pltpu.VMEM((8, 16, HALF), bf),
            pltpu.VMEM((8, 16, HALF), bf),
            pltpu.VMEM((NC, NCHIP, 16, HALF), bf),
            pltpu.VMEM((NCHIP, 16, HALF), bf),
            pltpu.VMEM((NCHIP, 16, HALF), bf),
            pltpu.VMEM((NCHIP, 16, HALF), f32),
            pltpu.VMEM((NCHIP, 16, HALF), bf),
            pltpu.VMEM((NCHIP, 16, HALF), bf),
            pltpu.VMEM((HEAD, 128), f32),
            pltpu.VMEM((8, 128), f32),
            pltpu.VMEM((HEAD, 128), f32),
            dma((2, 9)), dma((2, 9)),
            dma((2, 9, 4)), dma((2, 9, 4)),
            dma((4, 2)), dma((4, 2)),
            dma((2, 9)), dma((2, 9)),
            dma((8,)), dma((8,)),
            dma((NCHIP,)), dma((NCHIP,)),
            dma((NCHIP,)), dma((NCHIP,)),
            dma((NY,)), dma((NY,)),
            dma((NCHIP,)), dma((NCHIP,)),
        ],
        compiler_params=pltpu.CompilerParams(
            collective_id=0, has_side_effects=True
        ),
        name="layer",
    )(
        tokens.reshape(ROWS, D),
        queries.reshape(ROWS, 128),
        key_values.reshape(ROWS, 128),
        stop_bias.reshape(ROWS, 2).T,
        out_proj,
        norm_gain.reshape(1, D),
        up_proj,
        down_proj.T,
    )
    return out.reshape(8, 1, D)


def solution(mesh):
    return jax.shard_map(
        body,
        mesh=mesh,
        in_specs=(
            P("sp", None, None),
            P("sp", None, "tp"),
            P("sp", None, "tp"),
            P("sp", None, "tp"),
            P("tp", None),
            P(),
            P("sp", "tp"),
            P("tp", "sp"),
        ),
        out_specs=P(("sp", "tp"), None, None),
        check_vma=False,
    )
```

```python
import jax
import jax.numpy as jnp
from jax import lax
from jax.experimental import pallas as pl
from jax.experimental.pallas import tpu as pltpu
from jax.sharding import PartitionSpec as P

MESH = pl.DeviceIdType.MESH
NZ, NY, NX, NC = 16, 4, 4, 2
NCHIP = NX * NY
HEAD = 64
ROWS = 64
D = 2048
HALF = D // 2
EPSILON = 1e-06
LOG2E = 1.4426950408889634
UP_STEPS, DOWN_STEPS = 8, 7
JUMP = 4
W_PLAN = {0: ((1, 0),), 1: ((0, 0),), 2: ((1, 1),), 3: ((0, 1),), 5: ((1, 2),), 6: ((0, 2),), 7: ((1, 3), (0, 3))}


def nn(a, b):
    return lax.dot_general(a, b, (((1,), (0,)), ((), ())), preferred_element_type=jnp.float32)


def nt(a, b):
    return lax.dot_general(a, b, (((1,), (1,)), ((), ())), preferred_element_type=jnp.float32)


def tn(a, b):
    return lax.dot_general(a, b, (((0,), (0,)), ((), ())), preferred_element_type=jnp.float32)


def kernel(
    tok_hbm, q_hbm, kv_hbm, bias_hbm, wo_hbm, gain_hbm, up_hbm, down_hbm, out_ref,
    tok_ref, q_ref, bias_ref, wo_ref, gain_ref, up_ref, down_ref, in_s,
    kvall, wbuf, wcat, pbuf, prec, xbuf, e1, e1r, own, e2, erec,
    u_hi, s_hi, u_lo,
    kv_s, kv_r, yf_s, yf_r, we_s, we_r, w_s, w_r, p_s, p_r, x_s, x_r, xd_s, xd_r, e1_s, e1_r, e_s, e_r,
):
    sp = lax.axis_index("sp")
    tp = lax.axis_index("tp")
    z, y = sp // NY, sp % NY
    x, c = tp // NC, tp % NC
    chip = y * NX + x
    sibling = (sp, x * NC + 1 - c)

    def chip_at(r, core):
        dy, dx = r // NX, r % NX
        return (z * NY + (y + dy) % NY, ((x + dx) % NX) * NC + core)

    def rdma(src, dst, send, recv, device):
        return pltpu.make_async_remote_copy(
            src_ref=src, dst_ref=dst, send_sem=send, recv_sem=recv, device_id=device, device_id_type=MESH
        )

    barrier = pltpu.get_barrier_semaphore()
    peers = [(((z + d + NZ) % NZ) * NY + y, tp) for d in range(-JUMP, JUMP + 1) if d] + [sibling]
    peers += [chip_at(r, c) for r in range(1, NCHIP)]
    peers += [chip_at(r, 1 - c) for r in range(1, NX)]
    for peer in peers:
        pl.semaphore_signal(barrier, inc=1, device_id=peer, device_id_type=MESH)

    loads = [
        pltpu.make_async_copy(src, dst, in_s.at[i])
        for i, (src, dst) in enumerate(
            (
                (kv_hbm, kvall.at[z, y, 0:ROWS, :]),
                (bias_hbm, bias_ref),
                (up_hbm, up_ref),
                (down_hbm, down_ref),
                (q_hbm, q_ref),
                (wo_hbm, wo_ref),
                (tok_hbm.at[pl.ds(pl.multiple_of(tp * 8, 8), 8), :], tok_ref),
                (gain_hbm, gain_ref),
            )
        )
    ]
    for load in loads:
        load.start()

    loads[1].wait()
    bias = bias_ref[...].astype(jnp.float32)
    bias = jnp.concatenate([bias, jnp.zeros((6, HEAD), jnp.float32)], axis=0)
    bias = jnp.concatenate([bias, jnp.zeros((8, HEAD), jnp.float32)], axis=1)
    kvall[z, y, ROWS : ROWS + 8, :] = bias.astype(jnp.bfloat16)
    u_lo[...] = jnp.zeros_like(u_lo)

    loads[0].wait()
    pl.semaphore_wait(barrier, len(peers))

    def along(slot_of, send, recv, direction, d, held):
        hop = d - held
        if direction == 0:
            p, to = (z - held + NZ) % NZ, (z + hop) % NZ
        else:
            p, to = (z + held) % NZ, (z - hop + NZ) % NZ
        slot = slot_of(p)
        return rdma(slot, slot, send.at[direction, d], recv.at[direction, d], (to * NY + y, tp))

    def held_at(d):
        return (d - 1) // JUMP * JUMP

    def kv_copy(direction, d):
        return along(lambda p: kvall.at[p, y], kv_s, kv_r, direction, d, held_at(d))

    def used(direction, d):
        return (z - d >= 0) if direction == 0 else (z + d >= NZ) & (d <= DOWN_STEPS)

    def place(direction, d):
        return (z - d + NZ) % NZ if direction == 0 else (z + d) % NZ

    def kv_sends(direction, d):
        held = held_at(d)
        if direction == 0:
            return (z - held >= 0) & (z + d - held < NZ)
        if d % JUMP == 0:
            return (z + held) % NZ < DOWN_STEPS
        return (z - d + held + NZ) % NZ + d >= NZ

    def kv_arrives(direction, d):
        if direction == 1 and d % JUMP == 0:
            return (z + d) % NZ < DOWN_STEPS
        return used(direction, d)

    def kv_steps(direction):
        return range(1, (UP_STEPS, DOWN_STEPS)[direction] + 1)

    def kv_start(direction, d):
        @pl.when(kv_sends(direction, d))
        def _():
            kv_copy(direction, d).start()

    def kv_hand(direction, k, p, d, source=None):
        slot = kvall.at[p, y if source is None else source]
        return rdma(
            slot, slot, yf_s.at[direction, k, d], yf_r.at[direction, k, d], (z * NY + (y + d) % NY, tp)
        )

    def hand_start(direction, k, p):
        kv_hand(direction, k, p, 1).start()
        kv_hand(direction, k, p, 3).start()

        kv_hand(direction, k, p, 2).start()

    def hand_wait(direction, k, p):
        kv_hand(direction, k, p, 1).wait_recv()

        kv_hand(direction, k, p, 3).wait_recv()

        kv_hand(direction, k, p, 2).wait_recv()

    for d in range(JUMP, 0, -1):
        kv_start(0, d)
        kv_start(1, d)
    hand_start(0, 0, z)

    def w_hand(d, which):
        src = (up_ref, down_ref)[which]
        to = (y + d) % NY
        return rdma(
            src.at[:, pl.ds(pl.multiple_of(to * 128, 128), 128)],
            wbuf.at[z, which, pl.ds(pl.multiple_of(y * 32, 32), 32), :],
            we_s.at[d, which], we_r.at[d, which], (z * NY + to, tp),
        )

    loads[2].wait()
    loads[3].wait()
    for d in range(1, NY):
        for which in range(2):
            w_hand(d, which).start()
    for which in range(2):
        src = (up_ref, down_ref)[which]
        wbuf[z, which, pl.ds(pl.multiple_of(y * 32, 32), 32), :] = src[
            :, pl.ds(pl.multiple_of(y * 128, 128), 128)
        ]

    def w_copy(direction, d):
        return along(lambda p: wbuf.at[p], w_s, w_r, direction, d, (d - 1) // 2 * 2)

    def w_far(j, ways=(0, 1)):
        for direction in ways:
            last = (UP_STEPS, DOWN_STEPS)[direction]
            if 2 * j <= last:
                if j == 0:
                    if direction == ways[0]:
                        for d in range(1, NY):
                            for which in range(2):
                                w_hand(d, which).wait_recv()
                else:
                    w_copy(direction, 2 * j).wait_recv()
            if 2 * j + 2 <= last:
                w_copy(direction, 2 * j + 2).start()

    def w_near(j, ways=(0, 1)):
        for direction in ways:
            last = (UP_STEPS, DOWN_STEPS)[direction]
            if 2 * j + 1 <= last:
                w_copy(direction, 2 * j + 1).start()

    def w_work(point):
        for far, *step in W_PLAN.get(point, ()):
            (w_far if far else w_near)(*step)

    def w_rest():
        for d in range(1, UP_STEPS, 2):
            w_copy(0, d).wait_recv()
            w_copy(1, d).wait_recv()

    loads[4].wait()
    q = q_ref[...].astype(jnp.float32) * 0.125
    queries = jnp.concatenate([q[:, :HEAD], q[:, HEAD:]], axis=0).astype(jnp.bfloat16)
    pick = lax.broadcasted_iota(jnp.int32, (8, 128), 1) // HEAD
    pick = (pick == lax.broadcasted_iota(jnp.int32, (8, 128), 0)).astype(jnp.float32).astype(jnp.bfloat16)
    later = lax.broadcasted_iota(jnp.int32, (256, 256), 1) > lax.broadcasted_iota(jnp.int32, (256, 256), 0)
    later = later.astype(jnp.float32).astype(jnp.bfloat16)

    def attend(p, diagonal, carry):
        parts = []
        for b in range(NY):
            keys = kvall[p, b, 0:ROWS, 0:HEAD]
            biases = kvall[p, b, ROWS : ROWS + 8, 0:HEAD]
            parts.append(nt(keys, queries) + tn(biases, pick))
        score = jnp.concatenate(parts, axis=0) * LOG2E
        tail = jnp.log2(1.0 + jnp.exp2(-jnp.abs(score)))
        log_pass = -jnp.maximum(score, 0.0) - tail
        log_stop = jnp.minimum(score, 0.0) - tail
        if diagonal:
            key_at = lax.broadcasted_iota(jnp.int32, (256, 128), 0)
            query_at = y * ROWS + lax.broadcasted_iota(jnp.int32, (256, 128), 1) % HEAD
            strict = key_at < query_at
            log_pass = jnp.where(strict, log_pass, 0.0)
        high = log_pass.astype(jnp.bfloat16)
        low = (log_pass - high.astype(jnp.float32)).astype(jnp.bfloat16)
        after = nn(later, jnp.concatenate([high, low], axis=1))
        after = after[:, :128] + after[:, 128:]
        total = after[0:1, :] + log_pass[0:1, :]
        weights = jnp.exp2(log_stop + (after + carry))
        if diagonal:
            weights = jnp.where(strict, weights, 0.0)
        weights = weights.astype(jnp.bfloat16)
        values = jnp.concatenate([kvall[p, b, 0:ROWS, HEAD:128] for b in range(NY)], axis=0)
        return tn(values, weights), total

    def attend_diagonal():
        part, total = attend(z, True, 0.0)
        u_hi[...] = part
        s_hi[0:1, :] = total

    def attend_high(d):
        carry = s_hi[0:1, :]
        part, total = attend(place(0, d), False, carry)
        u_hi[...] += part
        s_hi[0:1, :] = carry + total

    def attend_both(d):
        carry = s_hi[0:1, :]
        part, total = attend(place(0, d), False, carry)
        part_low, total_low = attend(place(1, d), False, 0.0)
        u_hi[...] += part
        s_hi[0:1, :] = carry + total
        u_lo[...] = u_lo[...] * jnp.exp2(total_low) + part_low

    def kv_receive(d):
        for direction in range(2):
            if d in kv_steps(direction):
                @pl.when(kv_arrives(direction, d))
                def _():
                    kv_copy(direction, d).wait_recv()

                if d % JUMP == 0:
                    for further in range(d + JUMP, d, -1):
                        if further in kv_steps(direction):
                            kv_start(direction, further)

                @pl.when(used(direction, d))
                def _():
                    hand_start(direction, d, place(direction, d))

    def attend_step(d, unused):
        for direction in range(2):
            @pl.when(used(direction, d))
            def _():
                hand_wait(direction, d, place(direction, d))

        @pl.when(used(1, d))
        def _():
            attend_both(d)

        @pl.when(used(0, d) & jnp.logical_not(used(1, d)))
        def _():
            attend_high(d)

        return unused

    w_work(0)
    for d in (1, 2, 3, 4):
        kv_receive(d)
    w_work(1)
    hand_wait(0, 0, z)
    attend_diagonal()
    w_work(2)
    lax.fori_loop(1, 3, attend_step, 0)
    for d in (5, 6, 7, 8):
        kv_receive(d)
    w_work(3)
    lax.fori_loop(3, 5, attend_step, 0)
    w_work(4)
    w_work(5)
    lax.fori_loop(5, 9, attend_step, 0)
    w_work(6)

    for load in loads[5:]:
        load.wait()

    mixed = u_hi[...] + u_lo[...] * jnp.exp2(s_hi[0:1, :])
    mixed = mixed.T.astype(jnp.bfloat16)

    partial = nn(mixed[:ROWS], wo_ref[0:HEAD, :]) + nn(mixed[ROWS:], wo_ref[HEAD:, :])
    partial = partial.reshape(8, 8, D)
    pbuf[...] = jnp.concatenate([partial[:, :, :HALF], partial[:, :, HALF:]], axis=1).astype(jnp.bfloat16)

    def p_copy(r):
        to = (tp + r) % 8
        return rdma(pbuf.at[to], prec.at[r], p_s.at[r], p_r.at[r], (sp, to))

    for r in range(1, 8):
        p_copy(r).start()
    w_work(7)
    projected = pbuf[tp].astype(jnp.float32)
    for r in range(1, 8):
        p_copy(r).wait_recv()
        projected = projected + prec[r].astype(jnp.float32)
    projected = jnp.concatenate([projected[:8], projected[8:]], axis=1)
    residual = (tok_ref[...].astype(jnp.float32) + projected).astype(jnp.bfloat16).astype(jnp.float32)
    factor = lax.rsqrt(jnp.mean(residual * residual, axis=-1, keepdims=True) + EPSILON)
    normed = residual * factor * gain_ref[...]
    xbuf[c, chip] = jnp.concatenate([normed[:, :HALF], normed[:, HALF:]], axis=0).astype(jnp.bfloat16)

    def x_copy(r):
        slot = xbuf.at[c, chip]
        return rdma(slot, slot, x_s.at[r], x_r.at[r], chip_at(r, c))

    def x_pass(r):
        dy, dx = r // NX, r % NX
        source = ((y + NY - dy) % NY) * NX + (x + NX - dx) % NX
        slot = xbuf.at[c, source]
        return rdma(slot, slot, xd_s.at[r], xd_r.at[r], sibling)

    rows_order = (2, 1, 3, 0)
    for dy in rows_order:
        for dx in (2, 1, 3, 0):
            if dy or dx:
                x_copy(dy * NX + dx).start()
    x_pass(0).start()
    w_work(8)
    for dy in rows_order:
        for dx in (1, 3, 2, 0):
            if dy or dx:
                x_copy(dy * NX + dx).wait_recv()
                x_pass(dy * NX + dx).start()
    w_far(4)
    w_rest()
    for p in range(8):
        wcat[p * 128 : (p + 1) * 128, 0:128] = wbuf[p, 0]
        wcat[p * 128 : (p + 1) * 128, 128:256] = wbuf[p + 8, 0]

    def row_of(dy):
        return pl.ds(pl.multiple_of(((y + NY - dy) % NY) * NX, NX), NX)

    def swap(dy):
        rows = row_of(dy)
        return rdma(e1.at[rows], e1r.at[rows], e1_s.at[dy], e1_r.at[dy], sibling)

    def e_copy(r):
        dy, dx = r // NX, r % NX
        target = ((y + dy) % NY) * NX + (x + dx) % NX
        return rdma(e2.at[target], erec.at[r], e_s.at[r], e_r.at[r], chip_at(r, c))

    def feed_forward(pair):
        for dy in pair:
            for dx in range(NX):
                x_pass(dy * NX + dx).wait_recv()
        tokens = jnp.concatenate([xbuf[core, row_of(dy)] for dy in pair for core in (1 - c, c)], axis=0)
        both = nn(tokens.reshape(4 * NX * 16, HALF), wcat[...]).reshape(4 * NX, 16, 256)
        h = both[:, :8, :128] + both[:, 8:, 128:]
        h = jnp.maximum(h.reshape(4 * NX * 8, 128), 0.0)
        h = (h * h).astype(jnp.bfloat16)
        for p in range(8):
            w = jnp.concatenate([wbuf[p, 1], wbuf[p + 8, 1]], axis=0)
            o = nt(h, w).reshape(4 * NX, 8, 256)
            o = jnp.concatenate([o[:, :, :128], o[:, :, 128:]], axis=1)
            for n, dy in enumerate(pair):
                at = 2 * NX * n
                e1[row_of(dy), :, p * 128 : (p + 1) * 128] = o[at : at + NX].astype(jnp.bfloat16)
                own[row_of(dy), :, p * 128 : (p + 1) * 128] = o[at + NX : at + 2 * NX]
        for dy in pair:
            swap(dy).start()

    def send_back(dy):
        swap(dy).wait_recv()
        rows = row_of(dy)
        e2[rows] = (own[rows] + e1r[rows].astype(jnp.float32)).astype(jnp.bfloat16)
        for dx in (2, 1, 3, 0):
            r = ((NY - dy) % NY) * NX + dx
            if r:
                e_copy(r).start()

    feed_forward(rows_order[:2])
    send_back(rows_order[0])
    send_back(rows_order[1])
    feed_forward(rows_order[2:])
    send_back(rows_order[2])
    send_back(rows_order[3])
    update = own[chip] + e1r[chip].astype(jnp.float32)
    for dy in rows_order:
        for dx in range(NX):
            r = ((NY - dy) % NY) * NX + dx
            if r:
                e_copy(r).wait_recv()
                update = update + erec[r].astype(jnp.float32)
    update = jnp.concatenate([update[:8], update[8:]], axis=1)
    out_ref[...] = (residual + update).astype(jnp.bfloat16)

    for direction in range(2):
        for d in kv_steps(direction):
            @pl.when(kv_sends(direction, d))
            def _():
                kv_copy(direction, d).wait_send()

    def drain(k, unused):
        for direction in range(2):
            @pl.when(used(direction, k))
            def _():
                for d in range(1, NY):
                    kv_hand(direction, k, place(direction, k), d).wait_send()

        return unused

    lax.fori_loop(1, UP_STEPS + 1, drain, 0)
    for d in range(1, NY):
        kv_hand(0, 0, z, d).wait_send()
        for which in range(2):
            w_hand(d, which).wait_send()
    for k in range(1, UP_STEPS + 1):
        w_copy(0, k).wait_send()
    for k in range(1, DOWN_STEPS + 1):
        w_copy(1, k).wait_send()
    for r in range(1, 8):
        p_copy(r).wait_send()
    for r in range(NCHIP):
        x_pass(r).wait_send()
    for r in range(1, NCHIP):
        x_copy(r).wait_send()
        e_copy(r).wait_send()
    for dy in range(NY):
        swap(dy).wait_send()


def body(tokens, queries, key_values, stop_bias, out_proj, norm_gain, up_proj, down_proj):
    bf, f32 = jnp.bfloat16, jnp.float32
    dma = pltpu.SemaphoreType.DMA
    out = pl.pallas_call(
        kernel,
        out_shape=jax.ShapeDtypeStruct((8, D), bf),
        in_specs=[pl.BlockSpec(memory_space=pltpu.HBM)] * 8,
        out_specs=pl.BlockSpec(memory_space=pltpu.VMEM),
        scratch_shapes=[
            pltpu.VMEM((8, D), bf),
            pltpu.VMEM((ROWS, 128), bf),
            pltpu.VMEM((2, HEAD), bf),
            pltpu.VMEM((128, D), bf),
            pltpu.VMEM((1, D), f32),
            pltpu.VMEM((32, 512), bf),
            pltpu.VMEM((32, 512), bf),
            dma((8,)),
            pltpu.VMEM((NZ, NY, ROWS + 8, 128), bf),
            pltpu.VMEM((NZ, 2, 128, 128), bf),
            pltpu.VMEM((HALF, 256), bf),
            pltpu.VMEM((8, 16, HALF), bf),
            pltpu.VMEM((8, 16, HALF), bf),
            pltpu.VMEM((NC, NCHIP, 16, HALF), bf),
            pltpu.VMEM((NCHIP, 16, HALF), bf),
            pltpu.VMEM((NCHIP, 16, HALF), bf),
            pltpu.VMEM((NCHIP, 16, HALF), f32),
            pltpu.VMEM((NCHIP, 16, HALF), bf),
            pltpu.VMEM((NCHIP, 16, HALF), bf),
            pltpu.VMEM((HEAD, 128), f32),
            pltpu.VMEM((8, 128), f32),
            pltpu.VMEM((HEAD, 128), f32),
            dma((2, 9)), dma((2, 9)),
            dma((2, 9, 4)), dma((2, 9, 4)),
            dma((4, 2)), dma((4, 2)),
            dma((2, 9)), dma((2, 9)),
            dma((8,)), dma((8,)),
            dma((NCHIP,)), dma((NCHIP,)),
            dma((NCHIP,)), dma((NCHIP,)),
            dma((NY,)), dma((NY,)),
            dma((NCHIP,)), dma((NCHIP,)),
        ],
        compiler_params=pltpu.CompilerParams(
            collective_id=0, has_side_effects=True
        ),
        name="layer",
    )(
        tokens.reshape(ROWS, D),
        queries.reshape(ROWS, 128),
        key_values.reshape(ROWS, 128),
        stop_bias.reshape(ROWS, 2).T,
        out_proj,
        norm_gain.reshape(1, D),
        up_proj,
        down_proj.T,
    )
    return out.reshape(8, 1, D)


def solution(mesh):
    return jax.shard_map(
        body,
        mesh=mesh,
        in_specs=(
            P("sp", None, None),
            P("sp", None, "tp"),
            P("sp", None, "tp"),
            P("sp", None, "tp"),
            P("tp", None),
            P(),
            P("sp", "tp"),
            P("tp", "sp"),
        ),
        out_specs=P(("sp", "tp"), None, None),
        check_vma=False,
    )
```

```python
import jax
import jax.numpy as jnp
from jax import lax
from jax.experimental import pallas as pl
from jax.experimental.pallas import tpu as pltpu
from jax.sharding import PartitionSpec as P

MESH = pl.DeviceIdType.MESH
NZ, NY, NX, NC = 16, 4, 4, 2
NCHIP = NX * NY
HEAD = 64
ROWS = 64
D = 2048
HALF = D // 2
EPSILON = 1e-06
LOG2E = 1.4426950408889634
UP_STEPS, DOWN_STEPS = 8, 7
JUMP = 4
W_PLAN = {0: ((1, 0),), 1: ((0, 0),), 2: ((1, 1),), 3: ((0, 1),), 5: ((1, 2),), 6: ((0, 2),), 7: ((1, 3), (0, 3))}


def nn(a, b):
    return lax.dot_general(a, b, (((1,), (0,)), ((), ())), preferred_element_type=jnp.float32)


def nt(a, b):
    return lax.dot_general(a, b, (((1,), (1,)), ((), ())), preferred_element_type=jnp.float32)


def tn(a, b):
    return lax.dot_general(a, b, (((0,), (0,)), ((), ())), preferred_element_type=jnp.float32)


def kernel(
    tok_hbm, q_hbm, kv_hbm, bias_hbm, wo_hbm, gain_hbm, up_hbm, down_hbm, out_ref,
    tok_ref, q_ref, bias_ref, wo_ref, gain_ref, up_ref, down_ref, in_s,
    kvall, wbuf, wcat, pbuf, prec, xbuf, e1, e1r, own, e2, erec,
    u_hi, s_hi, u_lo,
    kv_s, kv_r, yf_s, yf_r, we_s, we_r, w_s, w_r, p_s, p_r, x_s, x_r, xd_s, xd_r, e1_s, e1_r, e_s, e_r,
):
    sp = lax.axis_index("sp")
    tp = lax.axis_index("tp")
    z, y = sp // NY, sp % NY
    x, c = tp // NC, tp % NC
    chip = y * NX + x
    sibling = (sp, x * NC + 1 - c)

    def chip_at(r, core):
        dy, dx = r // NX, r % NX
        return (z * NY + (y + dy) % NY, ((x + dx) % NX) * NC + core)

    def rdma(src, dst, send, recv, device):
        return pltpu.make_async_remote_copy(
            src_ref=src, dst_ref=dst, send_sem=send, recv_sem=recv, device_id=device, device_id_type=MESH
        )

    barrier = pltpu.get_barrier_semaphore()
    peers = [(((z + d + NZ) % NZ) * NY + y, tp) for d in range(-JUMP, JUMP + 1) if d] + [sibling]
    peers += [chip_at(r, c) for r in range(1, NCHIP)]
    peers += [chip_at(r, 1 - c) for r in range(1, NX)]
    for peer in peers:
        pl.semaphore_signal(barrier, inc=1, device_id=peer, device_id_type=MESH)

    loads = [
        pltpu.make_async_copy(src, dst, in_s.at[i])
        for i, (src, dst) in enumerate(
            (
                (kv_hbm, kvall.at[z, y, 0:ROWS, :]),
                (bias_hbm, bias_ref),
                (up_hbm, up_ref),
                (down_hbm, down_ref),
                (q_hbm, q_ref),
                (wo_hbm, wo_ref),
                (tok_hbm.at[pl.ds(pl.multiple_of(tp * 8, 8), 8), :], tok_ref),
                (gain_hbm, gain_ref),
            )
        )
    ]
    for load in loads:
        load.start()

    loads[1].wait()
    bias = bias_ref[...].astype(jnp.float32)
    bias = jnp.concatenate([bias, jnp.zeros((6, HEAD), jnp.float32)], axis=0)
    bias = jnp.concatenate([bias, jnp.zeros((8, HEAD), jnp.float32)], axis=1)
    kvall[z, y, ROWS : ROWS + 8, :] = bias.astype(jnp.bfloat16)
    u_lo[...] = jnp.zeros_like(u_lo)

    loads[0].wait()
    pl.semaphore_wait(barrier, len(peers))

    def along(slot_of, send, recv, direction, d, held):
        hop = d - held
        if direction == 0:
            p, to = (z - held + NZ) % NZ, (z + hop) % NZ
        else:
            p, to = (z + held) % NZ, (z - hop + NZ) % NZ
        slot = slot_of(p)
        return rdma(slot, slot, send.at[direction, d], recv.at[direction, d], (to * NY + y, tp))

    def held_at(d):
        return (d - 1) // JUMP * JUMP

    def kv_copy(direction, d):
        return along(lambda p: kvall.at[p, y], kv_s, kv_r, direction, d, held_at(d))

    def used(direction, d):
        return (z - d >= 0) if direction == 0 else (z + d >= NZ) & (d <= DOWN_STEPS)

    def place(direction, d):
        return (z - d + NZ) % NZ if direction == 0 else (z + d) % NZ

    def kv_sends(direction, d):
        held = held_at(d)
        if direction == 0:
            return (z - held >= 0) & (z + d - held < NZ)
        if d % JUMP == 0:
            return (z + held) % NZ < DOWN_STEPS
        return (z - d + held + NZ) % NZ + d >= NZ

    def kv_arrives(direction, d):
        if direction == 1 and d % JUMP == 0:
            return (z + d) % NZ < DOWN_STEPS
        return used(direction, d)

    def kv_steps(direction):
        return range(1, (UP_STEPS, DOWN_STEPS)[direction] + 1)

    def kv_start(direction, d):
        @pl.when(kv_sends(direction, d))
        def _():
            kv_copy(direction, d).start()

    def kv_hand(direction, k, p, d, source=None):
        slot = kvall.at[p, y if source is None else source]
        return rdma(
            slot, slot, yf_s.at[direction, k, d], yf_r.at[direction, k, d], (z * NY + (y + d) % NY, tp)
        )

    def hand_start(direction, k, p):
        kv_hand(direction, k, p, 1).start()
        kv_hand(direction, k, p, 3).start()

        kv_hand(direction, k, p, 2).start()

    def hand_wait(direction, k, p):
        kv_hand(direction, k, p, 1).wait_recv()

        kv_hand(direction, k, p, 3).wait_recv()

        kv_hand(direction, k, p, 2).wait_recv()

    for d in range(JUMP, 0, -1):
        kv_start(0, d)
        kv_start(1, d)
    hand_start(0, 0, z)

    def w_hand(d, which):
        src = (up_ref, down_ref)[which]
        to = (y + d) % NY
        return rdma(
            src.at[:, pl.ds(pl.multiple_of(to * 128, 128), 128)],
            wbuf.at[z, which, pl.ds(pl.multiple_of(y * 32, 32), 32), :],
            we_s.at[d, which], we_r.at[d, which], (z * NY + to, tp),
        )

    loads[2].wait()
    loads[3].wait()
    for d in range(1, NY):
        for which in range(2):
            w_hand(d, which).start()
    for which in range(2):
        src = (up_ref, down_ref)[which]
        wbuf[z, which, pl.ds(pl.multiple_of(y * 32, 32), 32), :] = src[
            :, pl.ds(pl.multiple_of(y * 128, 128), 128)
        ]

    def w_copy(direction, d):
        return along(lambda p: wbuf.at[p], w_s, w_r, direction, d, (d - 1) // 2 * 2)

    def w_far(j, ways=(0, 1)):
        for direction in ways:
            last = (UP_STEPS, DOWN_STEPS)[direction]
            if 2 * j <= last:
                if j == 0:
                    if direction == ways[0]:
                        for d in range(1, NY):
                            for which in range(2):
                                w_hand(d, which).wait_recv()
                else:
                    w_copy(direction, 2 * j).wait_recv()
            if 2 * j + 2 <= last:
                w_copy(direction, 2 * j + 2).start()

    def w_near(j, ways=(0, 1)):
        for direction in ways:
            last = (UP_STEPS, DOWN_STEPS)[direction]
            if 2 * j + 1 <= last:
                w_copy(direction, 2 * j + 1).start()

    def w_work(point):
        for far, *step in W_PLAN.get(point, ()):
            (w_far if far else w_near)(*step)

    def w_rest():
        for d in range(1, UP_STEPS, 2):
            w_copy(0, d).wait_recv()
            w_copy(1, d).wait_recv()

    loads[4].wait()
    q = q_ref[...].astype(jnp.float32) * 0.125
    queries = jnp.concatenate([q[:, :HEAD], q[:, HEAD:]], axis=0).astype(jnp.bfloat16)
    pick = lax.broadcasted_iota(jnp.int32, (8, 128), 1) // HEAD
    pick = (pick == lax.broadcasted_iota(jnp.int32, (8, 128), 0)).astype(jnp.float32).astype(jnp.bfloat16)
    later = lax.broadcasted_iota(jnp.int32, (256, 256), 1) > lax.broadcasted_iota(jnp.int32, (256, 256), 0)
    later = later.astype(jnp.float32).astype(jnp.bfloat16)

    def attend(p, diagonal, carry):
        parts = []
        for b in range(NY):
            keys = kvall[p, b, 0:ROWS, 0:HEAD]
            biases = kvall[p, b, ROWS : ROWS + 8, 0:HEAD]
            parts.append(nt(keys, queries) + tn(biases, pick))
        score = jnp.concatenate(parts, axis=0) * LOG2E
        tail = jnp.log2(1.0 + jnp.exp2(-jnp.abs(score)))
        log_pass = -jnp.maximum(score, 0.0) - tail
        log_stop = jnp.minimum(score, 0.0) - tail
        if diagonal:
            key_at = lax.broadcasted_iota(jnp.int32, (256, 128), 0)
            query_at = y * ROWS + lax.broadcasted_iota(jnp.int32, (256, 128), 1) % HEAD
            strict = key_at < query_at
            log_pass = jnp.where(strict, log_pass, 0.0)
        high = log_pass.astype(jnp.bfloat16)
        low = (log_pass - high.astype(jnp.float32)).astype(jnp.bfloat16)
        after = nn(later, jnp.concatenate([high, low], axis=1))
        after = after[:, :128] + after[:, 128:]
        total = after[0:1, :] + log_pass[0:1, :]
        weights = jnp.exp2(log_stop + (after + carry))
        if diagonal:
            weights = jnp.where(strict, weights, 0.0)
        weights = weights.astype(jnp.bfloat16)
        values = jnp.concatenate([kvall[p, b, 0:ROWS, HEAD:128] for b in range(NY)], axis=0)
        return tn(values, weights), total

    def attend_diagonal():
        part, total = attend(z, True, 0.0)
        u_hi[...] = part
        s_hi[0:1, :] = total

    def attend_high(d):
        carry = s_hi[0:1, :]
        part, total = attend(place(0, d), False, carry)
        u_hi[...] += part
        s_hi[0:1, :] = carry + total

    def attend_both(d):
        carry = s_hi[0:1, :]
        part, total = attend(place(0, d), False, carry)
        part_low, total_low = attend(place(1, d), False, 0.0)
        u_hi[...] += part
        s_hi[0:1, :] = carry + total
        u_lo[...] = u_lo[...] * jnp.exp2(total_low) + part_low

    def kv_receive(d):
        for direction in range(2):
            if d in kv_steps(direction):
                @pl.when(kv_arrives(direction, d))
                def _():
                    kv_copy(direction, d).wait_recv()

                if d % JUMP == 0:
                    for further in range(d + JUMP, d, -1):
                        if further in kv_steps(direction):
                            kv_start(direction, further)

                @pl.when(used(direction, d))
                def _():
                    hand_start(direction, d, place(direction, d))

    def attend_step(d, unused):
        for direction in range(2):
            @pl.when(used(direction, d))
            def _():
                hand_wait(direction, d, place(direction, d))

        @pl.when(used(1, d))
        def _():
            attend_both(d)

        @pl.when(used(0, d) & jnp.logical_not(used(1, d)))
        def _():
            attend_high(d)

        return unused

    w_work(0)
    for d in (1, 2, 3, 4):
        kv_receive(d)
    w_work(1)
    hand_wait(0, 0, z)
    attend_diagonal()
    w_work(2)
    lax.fori_loop(1, 3, attend_step, 0)
    for d in (5, 6, 7, 8):
        kv_receive(d)
    w_work(3)
    lax.fori_loop(3, 5, attend_step, 0)
    w_work(4)
    w_work(5)
    lax.fori_loop(5, 9, attend_step, 0)
    w_work(6)

    for load in loads[5:]:
        load.wait()

    mixed = u_hi[...] + u_lo[...] * jnp.exp2(s_hi[0:1, :])
    mixed = mixed.T.astype(jnp.bfloat16)

    partial = nn(mixed[:ROWS], wo_ref[0:HEAD, :]) + nn(mixed[ROWS:], wo_ref[HEAD:, :])
    partial = partial.reshape(8, 8, D)
    pbuf[...] = jnp.concatenate([partial[:, :, :HALF], partial[:, :, HALF:]], axis=1).astype(jnp.bfloat16)

    def p_copy(r):
        to = (tp + r) % 8
        return rdma(pbuf.at[to], prec.at[r], p_s.at[r], p_r.at[r], (sp, to))

    for r in (4, 5, 3, 2, 6, 7, 1):
        p_copy(r).start()
    w_work(7)
    projected = pbuf[tp].astype(jnp.float32)
    for r in (1, 7, 6, 2, 3, 5, 4):
        p_copy(r).wait_recv()
        projected = projected + prec[r].astype(jnp.float32)
    projected = jnp.concatenate([projected[:8], projected[8:]], axis=1)
    residual = (tok_ref[...].astype(jnp.float32) + projected).astype(jnp.bfloat16).astype(jnp.float32)
    factor = lax.rsqrt(jnp.mean(residual * residual, axis=-1, keepdims=True) + EPSILON)
    normed = residual * factor * gain_ref[...]
    xbuf[c, chip] = jnp.concatenate([normed[:, :HALF], normed[:, HALF:]], axis=0).astype(jnp.bfloat16)

    def x_copy(r):
        slot = xbuf.at[c, chip]
        return rdma(slot, slot, x_s.at[r], x_r.at[r], chip_at(r, c))

    def x_pass(r):
        dy, dx = r // NX, r % NX
        source = ((y + NY - dy) % NY) * NX + (x + NX - dx) % NX
        slot = xbuf.at[c, source]
        return rdma(slot, slot, xd_s.at[r], xd_r.at[r], sibling)

    rows_order = (2, 1, 3, 0)
    for dy in rows_order:
        for dx in (2, 1, 3, 0):
            if dy or dx:
                x_copy(dy * NX + dx).start()
    x_pass(0).start()
    w_work(8)
    for dy in rows_order:
        for dx in (1, 3, 2, 0):
            if dy or dx:
                x_copy(dy * NX + dx).wait_recv()
                x_pass(dy * NX + dx).start()
    w_far(4)
    w_rest()
    for p in range(8):
        wcat[p * 128 : (p + 1) * 128, 0:128] = wbuf[p, 0]
        wcat[p * 128 : (p + 1) * 128, 128:256] = wbuf[p + 8, 0]

    def row_of(dy):
        return pl.ds(pl.multiple_of(((y + NY - dy) % NY) * NX, NX), NX)

    def swap(dy):
        rows = row_of(dy)
        return rdma(e1.at[rows], e1r.at[rows], e1_s.at[dy], e1_r.at[dy], sibling)

    def e_copy(r):
        dy, dx = r // NX, r % NX
        target = ((y + dy) % NY) * NX + (x + dx) % NX
        return rdma(e2.at[target], erec.at[r], e_s.at[r], e_r.at[r], chip_at(r, c))

    def feed_forward(pair):
        for dy in pair:
            for dx in range(NX):
                x_pass(dy * NX + dx).wait_recv()
        tokens = jnp.concatenate([xbuf[core, row_of(dy)] for dy in pair for core in (1 - c, c)], axis=0)
        both = nn(tokens.reshape(4 * NX * 16, HALF), wcat[...]).reshape(4 * NX, 16, 256)
        h = both[:, :8, :128] + both[:, 8:, 128:]
        h = jnp.maximum(h.reshape(4 * NX * 8, 128), 0.0)
        h = (h * h).astype(jnp.bfloat16)
        for p in range(8):
            w = jnp.concatenate([wbuf[p, 1], wbuf[p + 8, 1]], axis=0)
            o = nt(h, w).reshape(4 * NX, 8, 256)
            o = jnp.concatenate([o[:, :, :128], o[:, :, 128:]], axis=1)
            for n, dy in enumerate(pair):
                at = 2 * NX * n
                e1[row_of(dy), :, p * 128 : (p + 1) * 128] = o[at : at + NX].astype(jnp.bfloat16)
                own[row_of(dy), :, p * 128 : (p + 1) * 128] = o[at + NX : at + 2 * NX]
        for dy in pair:
            swap(dy).start()

    def send_back(dy):
        swap(dy).wait_recv()
        rows = row_of(dy)
        e2[rows] = (own[rows] + e1r[rows].astype(jnp.float32)).astype(jnp.bfloat16)
        for dx in (2, 1, 3, 0):
            r = ((NY - dy) % NY) * NX + dx
            if r:
                e_copy(r).start()

    feed_forward(rows_order[:2])
    send_back(rows_order[0])
    send_back(rows_order[1])
    feed_forward(rows_order[2:])
    send_back(rows_order[2])
    send_back(rows_order[3])
    update = own[chip] + e1r[chip].astype(jnp.float32)
    for dy in rows_order:
        for dx in range(NX):
            r = ((NY - dy) % NY) * NX + dx
            if r:
                e_copy(r).wait_recv()
                update = update + erec[r].astype(jnp.float32)
    update = jnp.concatenate([update[:8], update[8:]], axis=1)
    out_ref[...] = (residual + update).astype(jnp.bfloat16)

    for direction in range(2):
        for d in kv_steps(direction):
            @pl.when(kv_sends(direction, d))
            def _():
                kv_copy(direction, d).wait_send()

    def drain(k, unused):
        for direction in range(2):
            @pl.when(used(direction, k))
            def _():
                for d in range(1, NY):
                    kv_hand(direction, k, place(direction, k), d).wait_send()

        return unused

    lax.fori_loop(1, UP_STEPS + 1, drain, 0)
    for d in range(1, NY):
        kv_hand(0, 0, z, d).wait_send()
        for which in range(2):
            w_hand(d, which).wait_send()
    for k in range(1, UP_STEPS + 1):
        w_copy(0, k).wait_send()
    for k in range(1, DOWN_STEPS + 1):
        w_copy(1, k).wait_send()
    for r in range(1, 8):
        p_copy(r).wait_send()
    for r in range(NCHIP):
        x_pass(r).wait_send()
    for r in range(1, NCHIP):
        x_copy(r).wait_send()
        e_copy(r).wait_send()
    for dy in range(NY):
        swap(dy).wait_send()


def body(tokens, queries, key_values, stop_bias, out_proj, norm_gain, up_proj, down_proj):
    bf, f32 = jnp.bfloat16, jnp.float32
    dma = pltpu.SemaphoreType.DMA
    out = pl.pallas_call(
        kernel,
        out_shape=jax.ShapeDtypeStruct((8, D), bf),
        in_specs=[pl.BlockSpec(memory_space=pltpu.HBM)] * 8,
        out_specs=pl.BlockSpec(memory_space=pltpu.VMEM),
        scratch_shapes=[
            pltpu.VMEM((8, D), bf),
            pltpu.VMEM((ROWS, 128), bf),
            pltpu.VMEM((2, HEAD), bf),
            pltpu.VMEM((128, D), bf),
            pltpu.VMEM((1, D), f32),
            pltpu.VMEM((32, 512), bf),
            pltpu.VMEM((32, 512), bf),
            dma((8,)),
            pltpu.VMEM((NZ, NY, ROWS + 8, 128), bf),
            pltpu.VMEM((NZ, 2, 128, 128), bf),
            pltpu.VMEM((HALF, 256), bf),
            pltpu.VMEM((8, 16, HALF), bf),
            pltpu.VMEM((8, 16, HALF), bf),
            pltpu.VMEM((NC, NCHIP, 16, HALF), bf),
            pltpu.VMEM((NCHIP, 16, HALF), bf),
            pltpu.VMEM((NCHIP, 16, HALF), bf),
            pltpu.VMEM((NCHIP, 16, HALF), f32),
            pltpu.VMEM((NCHIP, 16, HALF), bf),
            pltpu.VMEM((NCHIP, 16, HALF), bf),
            pltpu.VMEM((HEAD, 128), f32),
            pltpu.VMEM((8, 128), f32),
            pltpu.VMEM((HEAD, 128), f32),
            dma((2, 9)), dma((2, 9)),
            dma((2, 9, 4)), dma((2, 9, 4)),
            dma((4, 2)), dma((4, 2)),
            dma((2, 9)), dma((2, 9)),
            dma((8,)), dma((8,)),
            dma((NCHIP,)), dma((NCHIP,)),
            dma((NCHIP,)), dma((NCHIP,)),
            dma((NY,)), dma((NY,)),
            dma((NCHIP,)), dma((NCHIP,)),
        ],
        compiler_params=pltpu.CompilerParams(
            collective_id=0, has_side_effects=True
        ),
        name="layer",
    )(
        tokens.reshape(ROWS, D),
        queries.reshape(ROWS, 128),
        key_values.reshape(ROWS, 128),
        stop_bias.reshape(ROWS, 2).T,
        out_proj,
        norm_gain.reshape(1, D),
        up_proj,
        down_proj.T,
    )
    return out.reshape(8, 1, D)


def solution(mesh):
    return jax.shard_map(
        body,
        mesh=mesh,
        in_specs=(
            P("sp", None, None),
            P("sp", None, "tp"),
            P("sp", None, "tp"),
            P("sp", None, "tp"),
            P("tp", None),
            P(),
            P("sp", "tp"),
            P("tp", "sp"),
        ),
        out_specs=P(("sp", "tp"), None, None),
        check_vma=False,
    )
```

```python
import jax
import jax.numpy as jnp
from jax import lax
from jax.experimental import pallas as pl
from jax.experimental.pallas import tpu as pltpu
from jax.sharding import PartitionSpec as P

MESH = pl.DeviceIdType.MESH
NZ, NY, NX, NC = 16, 4, 4, 2
NCHIP = NX * NY
HEAD = 64
ROWS = 64
D = 2048
HALF = D // 2
EPSILON = 1e-06
LOG2E = 1.4426950408889634
UP_STEPS, DOWN_STEPS = 8, 7
JUMP = 4
W_PLAN = {0: ((1, 0),), 1: ((0, 0),), 2: ((1, 1),), 3: ((0, 1),), 5: ((1, 2), (0, 2)), 7: ((1, 3), (0, 3))}


def nn(a, b):
    return lax.dot_general(a, b, (((1,), (0,)), ((), ())), preferred_element_type=jnp.float32)


def nt(a, b):
    return lax.dot_general(a, b, (((1,), (1,)), ((), ())), preferred_element_type=jnp.float32)


def tn(a, b):
    return lax.dot_general(a, b, (((0,), (0,)), ((), ())), preferred_element_type=jnp.float32)


def kernel(
    tok_hbm, q_hbm, kv_hbm, bias_hbm, wo_hbm, gain_hbm, up_hbm, down_hbm, out_ref,
    tok_ref, q_ref, bias_ref, wo_ref, gain_ref, up_ref, down_ref, in_s,
    kvall, wbuf, wcat, pbuf, prec, xbuf, e1, e1r, own, e2, erec,
    u_hi, s_hi, u_lo,
    kv_s, kv_r, yf_s, yf_r, we_s, we_r, w_s, w_r, p_s, p_r, x_s, x_r, xd_s, xd_r, e1_s, e1_r, e_s, e_r,
):
    sp = lax.axis_index("sp")
    tp = lax.axis_index("tp")
    z, y = sp // NY, sp % NY
    x, c = tp // NC, tp % NC
    chip = y * NX + x
    sibling = (sp, x * NC + 1 - c)

    def chip_at(r, core):
        dy, dx = r // NX, r % NX
        return (z * NY + (y + dy) % NY, ((x + dx) % NX) * NC + core)

    def rdma(src, dst, send, recv, device):
        return pltpu.make_async_remote_copy(
            src_ref=src, dst_ref=dst, send_sem=send, recv_sem=recv, device_id=device, device_id_type=MESH
        )

    barrier = pltpu.get_barrier_semaphore()
    peers = [(((z + d + NZ) % NZ) * NY + y, tp) for d in range(-JUMP, JUMP + 1) if d] + [sibling]
    peers += [chip_at(r, c) for r in range(1, NCHIP)]
    peers += [chip_at(r, 1 - c) for r in range(1, NX)]
    for peer in peers:
        pl.semaphore_signal(barrier, inc=1, device_id=peer, device_id_type=MESH)

    loads = [
        pltpu.make_async_copy(src, dst, in_s.at[i])
        for i, (src, dst) in enumerate(
            (
                (kv_hbm, kvall.at[z, y, 0:ROWS, :]),
                (bias_hbm, bias_ref),
                (up_hbm, up_ref),
                (down_hbm, down_ref),
                (q_hbm, q_ref),
                (wo_hbm, wo_ref),
                (tok_hbm.at[pl.ds(pl.multiple_of(tp * 8, 8), 8), :], tok_ref),
                (gain_hbm, gain_ref),
            )
        )
    ]
    for load in loads:
        load.start()

    loads[1].wait()
    bias = bias_ref[...].astype(jnp.float32)
    bias = jnp.concatenate([bias, jnp.zeros((6, HEAD), jnp.float32)], axis=0)
    bias = jnp.concatenate([bias, jnp.zeros((8, HEAD), jnp.float32)], axis=1)
    kvall[z, y, ROWS : ROWS + 8, :] = bias.astype(jnp.bfloat16)
    u_lo[...] = jnp.zeros_like(u_lo)

    loads[0].wait()
    pl.semaphore_wait(barrier, len(peers))

    def along(slot_of, send, recv, direction, d, held):
        hop = d - held
        if direction == 0:
            p, to = (z - held + NZ) % NZ, (z + hop) % NZ
        else:
            p, to = (z + held) % NZ, (z - hop + NZ) % NZ
        slot = slot_of(p)
        return rdma(slot, slot, send.at[direction, d], recv.at[direction, d], (to * NY + y, tp))

    def held_at(d):
        return (d - 1) // JUMP * JUMP

    def kv_copy(direction, d):
        return along(lambda p: kvall.at[p, y], kv_s, kv_r, direction, d, held_at(d))

    def used(direction, d):
        return (z - d >= 0) if direction == 0 else (z + d >= NZ) & (d <= DOWN_STEPS)

    def place(direction, d):
        return (z - d + NZ) % NZ if direction == 0 else (z + d) % NZ

    def kv_sends(direction, d):
        held = held_at(d)
        if direction == 0:
            return (z - held >= 0) & (z + d - held < NZ)
        if d % JUMP == 0:
            return (z + held) % NZ < DOWN_STEPS
        return (z - d + held + NZ) % NZ + d >= NZ

    def kv_arrives(direction, d):
        if direction == 1 and d % JUMP == 0:
            return (z + d) % NZ < DOWN_STEPS
        return used(direction, d)

    def kv_steps(direction):
        return range(1, (UP_STEPS, DOWN_STEPS)[direction] + 1)

    def kv_start(direction, d):
        @pl.when(kv_sends(direction, d))
        def _():
            kv_copy(direction, d).start()

    def kv_hand(direction, k, p, d, source=None):
        slot = kvall.at[p, y if source is None else source]
        return rdma(
            slot, slot, yf_s.at[direction, k, d], yf_r.at[direction, k, d], (z * NY + (y + d) % NY, tp)
        )

    def hand_start(direction, k, p):
        kv_hand(direction, k, p, 1).start()
        kv_hand(direction, k, p, 3).start()

        kv_hand(direction, k, p, 2).start()

    def hand_wait(direction, k, p):
        kv_hand(direction, k, p, 1).wait_recv()

        kv_hand(direction, k, p, 3).wait_recv()

        kv_hand(direction, k, p, 2).wait_recv()

    for d in range(JUMP, 0, -1):
        kv_start(0, d)
        kv_start(1, d)
    hand_start(0, 0, z)

    def w_hand(d, which):
        src = (up_ref, down_ref)[which]
        to = (y + d) % NY
        return rdma(
            src.at[:, pl.ds(pl.multiple_of(to * 128, 128), 128)],
            wbuf.at[z, which, pl.ds(pl.multiple_of(y * 32, 32), 32), :],
            we_s.at[d, which], we_r.at[d, which], (z * NY + to, tp),
        )

    loads[2].wait()
    loads[3].wait()
    for d in range(1, NY):
        for which in range(2):
            w_hand(d, which).start()
    for which in range(2):
        src = (up_ref, down_ref)[which]
        wbuf[z, which, pl.ds(pl.multiple_of(y * 32, 32), 32), :] = src[
            :, pl.ds(pl.multiple_of(y * 128, 128), 128)
        ]

    def w_copy(direction, d):
        return along(lambda p: wbuf.at[p], w_s, w_r, direction, d, (d - 1) // 2 * 2)

    def w_far(j, ways=(0, 1)):
        for direction in ways:
            last = (UP_STEPS, DOWN_STEPS)[direction]
            if 2 * j <= last:
                if j == 0:
                    if direction == ways[0]:
                        for d in range(1, NY):
                            for which in range(2):
                                w_hand(d, which).wait_recv()
                else:
                    w_copy(direction, 2 * j).wait_recv()
            if 2 * j + 2 <= last:
                w_copy(direction, 2 * j + 2).start()

    def w_near(j, ways=(0, 1)):
        for direction in ways:
            last = (UP_STEPS, DOWN_STEPS)[direction]
            if 2 * j + 1 <= last:
                w_copy(direction, 2 * j + 1).start()

    def w_work(point):
        for far, *step in W_PLAN.get(point, ()):
            (w_far if far else w_near)(*step)

    def w_rest():
        for d in range(1, UP_STEPS, 2):
            w_copy(0, d).wait_recv()
            w_copy(1, d).wait_recv()

    loads[4].wait()
    q = q_ref[...].astype(jnp.float32) * 0.125
    queries = jnp.concatenate([q[:, :HEAD], q[:, HEAD:]], axis=0).astype(jnp.bfloat16)
    pick = lax.broadcasted_iota(jnp.int32, (8, 128), 1) // HEAD
    pick = (pick == lax.broadcasted_iota(jnp.int32, (8, 128), 0)).astype(jnp.float32).astype(jnp.bfloat16)
    later = lax.broadcasted_iota(jnp.int32, (256, 256), 1) > lax.broadcasted_iota(jnp.int32, (256, 256), 0)
    later = later.astype(jnp.float32).astype(jnp.bfloat16)

    def attend(p, diagonal, carry):
        parts = []
        for b in range(NY):
            keys = kvall[p, b, 0:ROWS, 0:HEAD]
            biases = kvall[p, b, ROWS : ROWS + 8, 0:HEAD]
            parts.append(nt(keys, queries) + tn(biases, pick))
        score = jnp.concatenate(parts, axis=0) * LOG2E
        tail = jnp.log2(1.0 + jnp.exp2(-jnp.abs(score)))
        log_pass = -jnp.maximum(score, 0.0) - tail
        log_stop = jnp.minimum(score, 0.0) - tail
        if diagonal:
            key_at = lax.broadcasted_iota(jnp.int32, (256, 128), 0)
            query_at = y * ROWS + lax.broadcasted_iota(jnp.int32, (256, 128), 1) % HEAD
            strict = key_at < query_at
            log_pass = jnp.where(strict, log_pass, 0.0)
        high = log_pass.astype(jnp.bfloat16)
        low = (log_pass - high.astype(jnp.float32)).astype(jnp.bfloat16)
        after = nn(later, jnp.concatenate([high, low], axis=1))
        after = after[:, :128] + after[:, 128:]
        total = after[0:1, :] + log_pass[0:1, :]
        weights = jnp.exp2(log_stop + (after + carry))
        if diagonal:
            weights = jnp.where(strict, weights, 0.0)
        weights = weights.astype(jnp.bfloat16)
        values = jnp.concatenate([kvall[p, b, 0:ROWS, HEAD:128] for b in range(NY)], axis=0)
        return tn(values, weights), total

    def attend_diagonal():
        part, total = attend(z, True, 0.0)
        u_hi[...] = part
        s_hi[0:1, :] = total

    def attend_high(d):
        carry = s_hi[0:1, :]
        part, total = attend(place(0, d), False, carry)
        u_hi[...] += part
        s_hi[0:1, :] = carry + total

    def attend_both(d):
        carry = s_hi[0:1, :]
        part, total = attend(place(0, d), False, carry)
        part_low, total_low = attend(place(1, d), False, 0.0)
        u_hi[...] += part
        s_hi[0:1, :] = carry + total
        u_lo[...] = u_lo[...] * jnp.exp2(total_low) + part_low

    def kv_receive(d):
        for direction in range(2):
            if d in kv_steps(direction):
                @pl.when(kv_arrives(direction, d))
                def _():
                    kv_copy(direction, d).wait_recv()

                if d % JUMP == 0:
                    for further in range(d + JUMP, d, -1):
                        if further in kv_steps(direction):
                            kv_start(direction, further)

                @pl.when(used(direction, d))
                def _():
                    hand_start(direction, d, place(direction, d))

    def attend_step(d, unused):
        for direction in range(2):
            @pl.when(used(direction, d))
            def _():
                hand_wait(direction, d, place(direction, d))

        @pl.when(used(1, d))
        def _():
            attend_both(d)

        @pl.when(used(0, d) & jnp.logical_not(used(1, d)))
        def _():
            attend_high(d)

        return unused

    w_work(0)
    for d in (1, 2, 3, 4):
        kv_receive(d)
    w_work(1)
    hand_wait(0, 0, z)
    attend_diagonal()
    w_work(2)
    lax.fori_loop(1, 3, attend_step, 0)
    for d in (5, 6, 7, 8):
        kv_receive(d)
    w_work(3)
    lax.fori_loop(3, 5, attend_step, 0)
    w_work(4)
    w_work(5)
    lax.fori_loop(5, 9, attend_step, 0)
    w_work(6)

    for load in loads[5:]:
        load.wait()

    mixed = u_hi[...] + u_lo[...] * jnp.exp2(s_hi[0:1, :])
    mixed = mixed.T.astype(jnp.bfloat16)

    partial = nn(mixed[:ROWS], wo_ref[0:HEAD, :]) + nn(mixed[ROWS:], wo_ref[HEAD:, :])
    partial = partial.reshape(8, 8, D)
    pbuf[...] = jnp.concatenate([partial[:, :, :HALF], partial[:, :, HALF:]], axis=1).astype(jnp.bfloat16)

    def p_copy(r):
        to = (tp + r) % 8
        return rdma(pbuf.at[to], prec.at[r], p_s.at[r], p_r.at[r], (sp, to))

    for r in (4, 5, 3, 2, 6, 7, 1):
        p_copy(r).start()
    w_work(7)
    projected = pbuf[tp].astype(jnp.float32)
    for r in (1, 7, 6, 2, 3, 5, 4):
        p_copy(r).wait_recv()
        projected = projected + prec[r].astype(jnp.float32)
    projected = jnp.concatenate([projected[:8], projected[8:]], axis=1)
    residual = (tok_ref[...].astype(jnp.float32) + projected).astype(jnp.bfloat16).astype(jnp.float32)
    factor = lax.rsqrt(jnp.mean(residual * residual, axis=-1, keepdims=True) + EPSILON)
    normed = residual * factor * gain_ref[...]
    xbuf[c, chip] = jnp.concatenate([normed[:, :HALF], normed[:, HALF:]], axis=0).astype(jnp.bfloat16)

    def x_copy(r):
        slot = xbuf.at[c, chip]
        return rdma(slot, slot, x_s.at[r], x_r.at[r], chip_at(r, c))

    def x_pass(r):
        dy, dx = r // NX, r % NX
        source = ((y + NY - dy) % NY) * NX + (x + NX - dx) % NX
        slot = xbuf.at[c, source]
        return rdma(slot, slot, xd_s.at[r], xd_r.at[r], sibling)

    rows_order = (2, 1, 3, 0)
    for dy in rows_order:
        for dx in (2, 1, 3, 0):
            if dy or dx:
                x_copy(dy * NX + dx).start()
    x_pass(0).start()
    w_work(8)
    for dy in rows_order:
        for dx in (1, 3, 2, 0):
            if dy or dx:
                x_copy(dy * NX + dx).wait_recv()
                x_pass(dy * NX + dx).start()
    w_far(4)
    w_rest()
    for p in range(8):
        wcat[p * 128 : (p + 1) * 128, 0:128] = wbuf[p, 0]
        wcat[p * 128 : (p + 1) * 128, 128:256] = wbuf[p + 8, 0]

    def row_of(dy):
        return pl.ds(pl.multiple_of(((y + NY - dy) % NY) * NX, NX), NX)

    def swap(dy):
        rows = row_of(dy)
        return rdma(e1.at[rows], e1r.at[rows], e1_s.at[dy], e1_r.at[dy], sibling)

    def e_copy(r):
        dy, dx = r // NX, r % NX
        target = ((y + dy) % NY) * NX + (x + dx) % NX
        return rdma(e2.at[target], erec.at[r], e_s.at[r], e_r.at[r], chip_at(r, c))

    def feed_forward(pair):
        for dy in pair:
            for dx in range(NX):
                x_pass(dy * NX + dx).wait_recv()
        tokens = jnp.concatenate([xbuf[core, row_of(dy)] for dy in pair for core in (1 - c, c)], axis=0)
        both = nn(tokens.reshape(4 * NX * 16, HALF), wcat[...]).reshape(4 * NX, 16, 256)
        h = both[:, :8, :128] + both[:, 8:, 128:]
        h = jnp.maximum(h.reshape(4 * NX * 8, 128), 0.0)
        h = (h * h).astype(jnp.bfloat16)
        for p in range(8):
            w = jnp.concatenate([wbuf[p, 1], wbuf[p + 8, 1]], axis=0)
            o = nt(h, w).reshape(4 * NX, 8, 256)
            o = jnp.concatenate([o[:, :, :128], o[:, :, 128:]], axis=1)
            for n, dy in enumerate(pair):
                at = 2 * NX * n
                e1[row_of(dy), :, p * 128 : (p + 1) * 128] = o[at : at + NX].astype(jnp.bfloat16)
                own[row_of(dy), :, p * 128 : (p + 1) * 128] = o[at + NX : at + 2 * NX]
        for dy in pair:
            swap(dy).start()

    def send_back(dy):
        swap(dy).wait_recv()
        rows = row_of(dy)
        e2[rows] = (own[rows] + e1r[rows].astype(jnp.float32)).astype(jnp.bfloat16)
        for dx in (2, 1, 3, 0):
            r = ((NY - dy) % NY) * NX + dx
            if r:
                e_copy(r).start()

    feed_forward(rows_order[:2])
    send_back(rows_order[0])
    feed_forward(rows_order[2:])
    send_back(rows_order[1])
    send_back(rows_order[2])
    send_back(rows_order[3])
    update = own[chip] + e1r[chip].astype(jnp.float32)
    for dy in rows_order:
        for dx in range(NX):
            r = ((NY - dy) % NY) * NX + dx
            if r:
                e_copy(r).wait_recv()
                update = update + erec[r].astype(jnp.float32)
    update = jnp.concatenate([update[:8], update[8:]], axis=1)
    out_ref[...] = (residual + update).astype(jnp.bfloat16)

    for direction in range(2):
        for d in kv_steps(direction):
            @pl.when(kv_sends(direction, d))
            def _():
                kv_copy(direction, d).wait_send()

    def drain(k, unused):
        for direction in range(2):
            @pl.when(used(direction, k))
            def _():
                for d in range(1, NY):
                    kv_hand(direction, k, place(direction, k), d).wait_send()

        return unused

    lax.fori_loop(1, UP_STEPS + 1, drain, 0)
    for d in range(1, NY):
        kv_hand(0, 0, z, d).wait_send()
        for which in range(2):
            w_hand(d, which).wait_send()
    for k in range(1, UP_STEPS + 1):
        w_copy(0, k).wait_send()
    for k in range(1, DOWN_STEPS + 1):
        w_copy(1, k).wait_send()
    for r in range(1, 8):
        p_copy(r).wait_send()
    for r in range(NCHIP):
        x_pass(r).wait_send()
    for r in range(1, NCHIP):
        x_copy(r).wait_send()
        e_copy(r).wait_send()
    for dy in range(NY):
        swap(dy).wait_send()


def body(tokens, queries, key_values, stop_bias, out_proj, norm_gain, up_proj, down_proj):
    bf, f32 = jnp.bfloat16, jnp.float32
    dma = pltpu.SemaphoreType.DMA
    out = pl.pallas_call(
        kernel,
        out_shape=jax.ShapeDtypeStruct((8, D), bf),
        in_specs=[pl.BlockSpec(memory_space=pltpu.HBM)] * 8,
        out_specs=pl.BlockSpec(memory_space=pltpu.VMEM),
        scratch_shapes=[
            pltpu.VMEM((8, D), bf),
            pltpu.VMEM((ROWS, 128), bf),
            pltpu.VMEM((2, HEAD), bf),
            pltpu.VMEM((128, D), bf),
            pltpu.VMEM((1, D), f32),
            pltpu.VMEM((32, 512), bf),
            pltpu.VMEM((32, 512), bf),
            dma((8,)),
            pltpu.VMEM((NZ, NY, ROWS + 8, 128), bf),
            pltpu.VMEM((NZ, 2, 128, 128), bf),
            pltpu.VMEM((HALF, 256), bf),
            pltpu.VMEM((8, 16, HALF), bf),
            pltpu.VMEM((8, 16, HALF), bf),
            pltpu.VMEM((NC, NCHIP, 16, HALF), bf),
            pltpu.VMEM((NCHIP, 16, HALF), bf),
            pltpu.VMEM((NCHIP, 16, HALF), bf),
            pltpu.VMEM((NCHIP, 16, HALF), f32),
            pltpu.VMEM((NCHIP, 16, HALF), bf),
            pltpu.VMEM((NCHIP, 16, HALF), bf),
            pltpu.VMEM((HEAD, 128), f32),
            pltpu.VMEM((8, 128), f32),
            pltpu.VMEM((HEAD, 128), f32),
            dma((2, 9)), dma((2, 9)),
            dma((2, 9, 4)), dma((2, 9, 4)),
            dma((4, 2)), dma((4, 2)),
            dma((2, 9)), dma((2, 9)),
            dma((8,)), dma((8,)),
            dma((NCHIP,)), dma((NCHIP,)),
            dma((NCHIP,)), dma((NCHIP,)),
            dma((NY,)), dma((NY,)),
            dma((NCHIP,)), dma((NCHIP,)),
        ],
        compiler_params=pltpu.CompilerParams(
            collective_id=0, has_side_effects=True
        ),
        name="layer",
    )(
        tokens.reshape(ROWS, D),
        queries.reshape(ROWS, 128),
        key_values.reshape(ROWS, 128),
        stop_bias.reshape(ROWS, 2).T,
        out_proj,
        norm_gain.reshape(1, D),
        up_proj,
        down_proj.T,
    )
    return out.reshape(8, 1, D)


def solution(mesh):
    return jax.shard_map(
        body,
        mesh=mesh,
        in_specs=(
            P("sp", None, None),
            P("sp", None, "tp"),
            P("sp", None, "tp"),
            P("sp", None, "tp"),
            P("tp", None),
            P(),
            P("sp", "tp"),
            P("tp", "sp"),
        ),
        out_specs=P(("sp", "tp"), None, None),
        check_vma=False,
    )
```
